512 devices in a mesh: grp: 2 (over y), sp: 32 (over z), tp: 8 (over x, core).
Axes of the slice: x: 4, y: 2, z: 32, core: 2. Of those that a mesh axis runs over, the one named last changes fastest.
The devices are a block of a 4x8x32 slice.
Arguments:
- latent: bfloat16 [16384, 4096], P(('grp', 'sp')), parts along dimension 0, may hold values from -6 to 6
- context: bfloat16 [512, 4096], P(('grp', 'sp')), parts along dimension 0, may hold values from -6 to 6
- cond_latent: float32 [8192], P(('grp', 'sp')), parts along dimension 0, may hold values from -6 to 6
- cond_context: float32 [8192], P(('grp', 'sp')), parts along dimension 0, may hold values from -6 to 6
- mod_weight: bfloat16 [3, 4096, 4096], P(None, 'sp', 'tp'), may hold values from -0.09375 to 0.09375
- norm_gain: float32 [4096], replicated, may hold values from 0.1 to 1.9
- w_query: bfloat16 [4096, 1024], P('sp', 'tp'), may hold values from -0.09375 to 0.09375
- w_key: bfloat16 [4096, 1024], P('sp', 'tp'), may hold values from -0.09375 to 0.09375
- w_value: bfloat16 [4096, 2048], P('sp', 'tp'), may hold values from -0.09375 to 0.09375
- w_rank: bfloat16 [2, 4096, 64], P(None, 'sp'), may hold values from -0.09375 to 0.09375
- w_decay: bfloat16 [2, 64, 1024], P(None, None, 'tp'), may hold values from -0.75 to 0.75
- decay_bias: float32 [2, 1024], P(None, 'tp'), may hold values from -1 to 20
- decay_shift: float32 [16384, 16], P(('grp', 'sp'), 'tp'), parts along dimension 0, may hold values from -1 to 0
- out_gain: float32 [2048], P('tp'), may hold values from 0.1 to 1.9
- w_out: bfloat16 [2048, 4096], P('tp', 'sp'), may hold values from -0.125 to 0.125
Outputs:
- mixed: bfloat16 [16384, 4096], P(('grp', 'sp')), parts along dimension 0
The draws below stay inside these ranges and needn't reach their ends.
There are 2 independent parts, one for each index of `grp`. The reference program is written for one: setup_inputs(seed, part) draws one part's arguments, and reference() takes and returns one part's arrays. A program takes and returns all parts, laid end to end along the dimension named above; an argument that names none is the same for every part. Nothing has to cross between parts.
All inputs are finite; a program needn't handle non-finite values.
Results may differ from the reference program's by a relative error of at most 0.0095.
Values may be sent and summed in bfloat16 or wider, within the bound.
No kernel may reach another device: no remote copies, remote signals or barrier semaphores. Data moves between devices by JAX's collectives and lax.ppermute only.
A program may use at most 128 MiB of HBM per device.

```python
import jax
import jax.numpy as jnp
from jax import lax

D = 4096
HEAD_TOTAL = 16
DK = 64
DV = 128
RANK = 64
BLOCK = 64
L_DEV = 256
CTX = 256
LATENT_TOKENS = 8192
QK = 1024
WIDTH = 2048
GROUPS = 8


def draw_decay_bias(key, part):
    key_mask, key_fast, key_slow = jax.random.split(jax.random.fold_in(key, 11), 3)
    fast_head = jax.random.uniform(key_mask, (2, HEAD_TOTAL)) < 0.5
    fast_values = jax.random.uniform(key_fast, (2, QK), minval=-0.5, maxval=1.0)
    slow_values = jnp.log(LATENT_TOKENS / 4.8) + jax.random.uniform(key_slow, (2, QK), minval=-0.5, maxval=0.5)
    chosen = jnp.repeat(fast_head, DK, axis=1)
    return jnp.where(chosen, fast_values, slow_values).astype(jnp.float32)


def draw_decay_shift(key, part):
    key_speed, key_spike, key_level = jax.random.split(jax.random.fold_in(key, 23), 3)
    segments = LATENT_TOKENS // L_DEV
    rates = jnp.exp(jax.random.uniform(key_speed, (segments, 1, HEAD_TOTAL), minval=jnp.log(0.2), maxval=jnp.log(0.8)))
    baseline = -jnp.broadcast_to(rates, (segments, L_DEV, HEAD_TOTAL)).reshape(LATENT_TOKENS, HEAD_TOTAL) / LATENT_TOKENS
    struck_entries = jax.random.uniform(key_spike, (LATENT_TOKENS, HEAD_TOTAL)) < 2.0 / LATENT_TOKENS
    depths = jnp.log(jax.random.uniform(key_level, (LATENT_TOKENS, HEAD_TOTAL), minval=0.5, maxval=0.8))
    return (baseline + jnp.where(struck_entries, depths, 0.0)).astype(jnp.float32)


def block_levels(own_key, dims, shards, least, top_value):
    def one(dim, parts):
        steps = jax.random.uniform(jax.random.fold_in(jax.random.fold_in(own_key, 6), dim), (parts,), jnp.float32, least / len(shards), top_value / len(shards))
        return jnp.repeat(jnp.exp(steps), dims[dim] // parts).reshape((-1,) + (1,) * (len(dims) - dim - 1))

    loudness = one(*shards[0])
    for cut in shards[1:]:
        loudness = loudness * one(*cut)
    return loudness


def centred(own_key, dims, spread, bound, cuts=(), kind=jnp.bfloat16):
    drawn = spread * jax.random.normal(own_key, dims, jnp.float32)
    if cuts:
        drawn = drawn * block_levels(own_key, dims, cuts, -0.22, 0.18)
    return jnp.clip(drawn, -bound, bound).astype(kind)


def setup_inputs(seed: int = 0, part: int = 0) -> dict:
    arg_keys = jax.random.split(jax.random.key(seed), 16)
    part_splits = jax.random.split(jax.random.fold_in(arg_keys[15], part), 16)
    latent = centred(part_splits[0], (LATENT_TOKENS, D), 1.0, 6.0, ((0, 32),))
    context = centred(part_splits[1], (CTX, D), 1.0, 6.0, ((0, 32),))
    cond_latent = centred(part_splits[2], (D,), 1.0, 6.0, ((0, 32),), jnp.float32)
    cond_context = centred(part_splits[3], (D,), 1.0, 6.0, ((0, 32),), jnp.float32)
    mod_weight = centred(arg_keys[4], (3, D, D), D ** -0.5, 0.09375, ((1, 32), (2, 8)))
    norm_gain = jnp.clip(1.0 + 0.18 * jax.random.normal(arg_keys[5], (D,), jnp.float32), 0.1, 1.9)
    w_query = centred(arg_keys[6], (D, QK), D ** -0.5, 0.09375, ((0, 32), (1, 8)))
    w_key = centred(arg_keys[7], (D, QK), D ** -0.5, 0.09375, ((0, 32), (1, 8)))
    w_value = centred(arg_keys[8], (D, WIDTH), D ** -0.5, 0.09375, ((0, 32), (1, 8)))
    w_rank = centred(arg_keys[9], (2, D, RANK), D ** -0.5, 0.09375, ((1, 32),))
    w_decay = centred(arg_keys[10], (2, RANK, QK), RANK ** -0.5, 0.75, ((2, 8),))
    decay_bias = draw_decay_bias(jax.random.fold_in(arg_keys[15], 71), part)
    decay_shift = draw_decay_shift(jax.random.fold_in(jax.random.fold_in(arg_keys[15], part), 71), part)
    out_gain = jnp.clip(1.0 + 0.18 * jax.random.normal(arg_keys[13], (WIDTH,), jnp.float32), 0.1, 1.9)
    w_out = centred(arg_keys[14], (WIDTH, D), WIDTH ** -0.5, 0.125, ((0, 8), (1, 32)))
    return {"latent": latent, "context": context, "cond_latent": cond_latent, "cond_context": cond_context, "mod_weight": mod_weight, "norm_gain": norm_gain, "w_query": w_query, "w_key": w_key, "w_value": w_value, "w_rank": w_rank, "w_decay": w_decay, "decay_bias": decay_bias, "decay_shift": decay_shift, "out_gain": out_gain, "w_out": w_out}


eps = 1e-06
normalizer = 16.0
precise = lax.Precision.HIGHEST

def rounded(tensor):
    return lax.optimization_barrier(tensor.astype(jnp.bfloat16))

def modulated(tokens, norm_gain, shift_row, scale_row):
    widened = tokens.astype(jnp.float32)
    normalized = widened * lax.rsqrt(lax.optimization_barrier(jnp.mean(widened * widened, axis=-1, keepdims=True)) + eps)
    return (normalized * norm_gain * (1.0 + scale_row) + shift_row).astype(jnp.bfloat16)

def project(tokens, weight):
    return rounded(jnp.dot(tokens, weight, preferred_element_type=jnp.float32))

def log_decay(rank_rows, weight, bias):
    return jax.nn.log_sigmoid(jnp.dot(rank_rows, weight, preferred_element_type=jnp.float32) + bias) / normalizer

def by_heads(tensor, width):
    return tensor.astype(jnp.float32).reshape(tensor.shape[0], -1, width)

def context_state(key_rows, value_rows, decays, forward):
    running = jnp.cumsum(decays, axis=0)
    if forward:
        factor = jnp.exp(running[-1] - running)
    else:
        factor = jnp.exp(running - decays)
    return jnp.einsum('thd,the->hde', key_rows * factor, value_rows, precision=precise)

def chain(queries, key_rows, value_rows, decays, initial):
    length, head_count, _ = queries.shape
    blocks = length // BLOCK
    lower_mask = jnp.tril(jnp.ones((BLOCK, BLOCK), dtype=bool))

    def in_blocks(tensor):
        return tensor.reshape(blocks, BLOCK, head_count, tensor.shape[-1])

    def advance(carry_state, inputs):
        query_block, key_block, value_block, decay_block = inputs
        running = jnp.cumsum(decay_block, axis=0)
        carried = jnp.einsum('chd,hde->che', query_block * jnp.exp(running), carry_state, precision=precise)
        relative = jnp.where(lower_mask[:, :, None, None], running[:, None] - running[None, :], -jnp.inf)
        scores = jnp.einsum('ihd,jhd,ijhd->ijh', query_block, key_block, jnp.exp(relative), precision=precise)
        within = jnp.einsum('ijh,jhe->ihe', scores, value_block, precision=precise)
        block_total = running[-1]
        carry_state = jnp.exp(block_total)[:, :, None] * carry_state + jnp.einsum('chd,che->hde', key_block * jnp.exp(block_total - running), value_block, precision=precise)
        return (carry_state, carried + within)
    _, outputs = lax.scan(advance, initial, (in_blocks(queries), in_blocks(key_rows), in_blocks(value_rows), in_blocks(decays)))
    return outputs.reshape(length, head_count, value_rows.shape[-1])

def reference(latent, context, cond_latent, cond_context, mod_weight, norm_gain, w_query, w_key, w_value, w_rank, w_decay, decay_bias, decay_shift, out_gain, w_out):
    silu_latent = rounded(jax.nn.silu(cond_latent))
    silu_context = rounded(jax.nn.silu(cond_context))
    widened_mod = mod_weight.astype(jnp.float32)
    mod_latent = jnp.einsum('d,rdc->rc', silu_latent.astype(jnp.float32), widened_mod, precision=precise)
    mod_context = jnp.einsum('d,rdc->rc', silu_context.astype(jnp.float32), widened_mod[:2], precision=precise)
    h_latent = modulated(latent, norm_gain, mod_latent[0], mod_latent[1])
    h_context = modulated(context, norm_gain, mod_context[0], mod_context[1])
    queries = by_heads(project(h_latent, w_query), DK)
    key_rows = by_heads(project(h_latent, w_key), DK)
    value_rows = by_heads(project(h_latent, w_value), DV)
    shift_rows = decay_shift[:, :, None]
    log_fwd = by_heads(log_decay(project(h_latent, w_rank[0]), w_decay[0], decay_bias[0]), DK) + shift_rows
    log_bwd = by_heads(log_decay(project(h_latent, w_rank[1]), w_decay[1], decay_bias[1]), DK) + shift_rows
    context_keys = by_heads(project(h_context, w_key), DK)
    context_values = by_heads(project(h_context, w_value), DV)
    context_fwd = by_heads(log_decay(project(h_context, w_rank[0]), w_decay[0], decay_bias[0]), DK)
    context_bwd = by_heads(log_decay(project(h_context, w_rank[1]), w_decay[1], decay_bias[1]), DK)
    start_fwd = context_state(context_keys, context_values, context_fwd, True)
    start_bwd = context_state(context_keys, context_values, context_bwd, False)
    out_fwd = chain(queries, key_rows, value_rows, log_fwd, start_fwd)
    out_bwd = jnp.flip(chain(jnp.flip(queries, 0), jnp.flip(key_rows, 0), jnp.flip(value_rows, 0), jnp.flip(log_bwd, 0), start_bwd), 0)
    combined = out_fwd + out_bwd
    combined = combined * lax.rsqrt(lax.optimization_barrier(jnp.mean(combined * combined, axis=-1, keepdims=True)) + eps)
    normed = (combined.reshape(combined.shape[0], -1) * out_gain).astype(jnp.bfloat16)
    group_width = normed.shape[1] // GROUPS
    summed = jnp.zeros((normed.shape[0], w_out.shape[1]), jnp.float32)
    for group in range(GROUPS):
        lower_edge = group * group_width
        part = rounded(jnp.dot(normed[:, lower_edge:lower_edge + group_width], w_out[lower_edge:lower_edge + group_width], preferred_element_type=jnp.float32))
        summed = summed + part.astype(jnp.float32)
    return (latent.astype(jnp.float32) + mod_latent[2] * summed).astype(jnp.bfloat16)
```

```python
import jax
import jax.numpy as jnp
from jax import lax
from jax.experimental import pallas as pl
from jax.experimental.pallas import tpu as pltpu
from jax.sharding import PartitionSpec as P

DK = 64
DV = 128
eps = 1e-06
normalizer = 16.0
f32 = jnp.float32
bf16 = jnp.bfloat16
VMEM_LIMIT = 50 * 1024 * 1024


def sent_to_all(array, axis):
    copies = jnp.broadcast_to(array, (lax.axis_size(axis), *array.shape))
    return lax.all_to_all(copies, axis, split_axis=0, concat_axis=0, tiled=True)


def dot(a, b):
    return jnp.dot(a, b, preferred_element_type=f32)


def dot_nt(a, b):
    return lax.dot_general(a, b, (((1,), (1,)), ((), ())), preferred_element_type=f32)


def dot_tn(a, b):
    return lax.dot_general(a, b, (((0,), (0,)), ((), ())), preferred_element_type=f32)


def halves(x):
    high = x.astype(bf16)
    low = (x - high.astype(f32)).astype(bf16)
    return high, low


def iota(shape, dim):
    return lax.broadcasted_iota(jnp.int32, shape, dim)


def log_sigmoid(u):
    return jnp.minimum(u, 0.0) - jnp.log1p(jnp.exp(-jnp.abs(u)))


def head_state(keys, values):
    both = dot_tn(keys, values)
    rows = iota((2 * DK, DV), 0)
    return jnp.where(rows < DK, both[:, :DV], both[:, DV:])


def mixing_kernel(
    h_ref, wqk_ref, wv_ref, wr_ref, wd_ref, bias_ref, shift_ref,
    loc_ref, lift_ref, send_ref, acc,
):
    step = pl.program_id(0)
    T = shift_ref.shape[0]
    C = h_ref.shape[0] - T
    h = h_ref[...]

    @pl.when(step == 0)
    def _():
        acc[...] = jnp.zeros_like(acc)

    acc[:, 0:256] += dot(h, wqk_ref[...])
    acc[:, 256:512] += dot(h, wv_ref[...])
    acc[:, 512:640] += dot(h, wr_ref[...])

    @pl.when(step == pl.num_programs(0) - 1)
    def _():
        q16 = acc[0:T, 0:128].astype(bf16)
        k16 = acc[0:T, 128:256].astype(bf16)
        v = acc[0:T, 256:512].astype(bf16)
        q = q16.astype(f32)
        k = k16.astype(f32)
        ranks = acc[:, 512:640].astype(bf16)
        logs = log_sigmoid(dot(ranks, wd_ref[...]) + bias_ref[...]) / normalizer
        lat = logs[0:T] + shift_ref[...]
        f_high, f_low = halves(lat[:, 0:128])
        b_high, b_low = halves(lat[:, 128:256])
        f_pair = jnp.concatenate([f_high, f_low], axis=1)
        b_pair = jnp.concatenate([b_high, b_low], axis=1)

        def summed(where, pair):
            both = dot(jnp.where(where, 1.0, 0.0).astype(bf16), pair)
            return both[:, 0:128] + both[:, 128:256]

        r = iota((T, T), 0)
        s = iota((T, T), 1)
        lane = iota((T, 128), 1)
        row = iota((T, 128), 0)
        first = lane < DK
        zero = jnp.zeros((T, 128), bf16)

        def scores(qs, ks):
            return (
                dot_nt(qs, jnp.where(first, ks, zero)),
                dot_nt(qs, jnp.where(first, zero, ks)),
            )

        s0, s1 = scores(q16, k16)
        s0 = 2.0 * s0
        s1 = 2.0 * s1
        m = 1
        while m < T:
            base = (r // (2 * m)) * (2 * m)
            ref = base + m
            upper = r >= ref
            lower = r < ref
            d_f = (upper & (s >= ref) & (s <= r)) | (lower & (s > r) & (s < ref))
            d_b = (upper & (s >= ref) & (s < r)) | (lower & (s >= r) & (s < ref))
            fac_f = jnp.exp(summed(d_f, f_pair))
            fac_b = jnp.exp(summed(d_b, b_pair))
            up = (row & m) != 0
            qs = (q * jnp.where(up, fac_f, fac_b)).astype(bf16)
            ks = (k * jnp.where(up, fac_b, fac_f)).astype(bf16)
            m0, m1 = scores(qs, ks)
            pick = ((r ^ s) >= m) & ((r ^ s) < 2 * m)
            s0 = jnp.where(pick, m0, s0)
            s1 = jnp.where(pick, m1, s1)
            m *= 2
        loc_ref[:, 0:128] = dot(s0.astype(bf16), v[:, 0:128])
        loc_ref[:, 128:256] = dot(s1.astype(bf16), v[:, 128:256])

        lift_ref[:, 0:128] = (q * jnp.exp(summed(s <= r, f_pair))).astype(bf16)
        lift_ref[:, 128:256] = (q * jnp.exp(summed(s >= r, b_pair))).astype(bf16)
        k_f = (k * jnp.exp(summed(s > r, f_pair))).astype(bf16)
        k_b = (k * jnp.exp(summed(s < r, b_pair))).astype(bf16)

        def total(high, low):
            ones = jnp.ones((high.shape[0], 128), bf16)
            return jnp.exp(dot_tn(high, ones) + dot_tn(low, ones))

        n = send_ref.shape[0]
        st_f = head_state(k_f, v)
        st_b = head_state(k_b, v)
        half = n // 2
        send_ref[0:half, 0:8, :] = st_f.reshape(half, 8, 128).astype(bf16)
        send_ref[half:n, 0:8, :] = st_b.reshape(half, 8, 128).astype(bf16)

        crow = iota((C, 128), 0)
        live = crow < 8
        kc = jnp.where(live, acc[T : T + C, 128:256].astype(bf16).astype(f32), 0.0)
        vc = acc[T : T + C, 256:512].astype(bf16)
        ctx_f = jnp.where(live, logs[T : T + C, 0:128], 0.0)
        ctx_b = jnp.where(live, logs[T : T + C, 128:256], 0.0)
        cf_high, cf_low = halves(ctx_f)
        cb_high, cb_low = halves(ctx_b)
        rc = iota((C, C), 0)
        sc = iota((C, C), 1)
        kc_f = (kc * jnp.exp(summed(sc > rc, jnp.concatenate([cf_high, cf_low], axis=1)))).astype(bf16)
        kc_b = (kc * jnp.exp(summed(sc < rc, jnp.concatenate([cb_high, cb_low], axis=1)))).astype(bf16)
        send_ref[0:half, 8:16, :] = head_state(kc_f, vc).reshape(half, 8, 128).astype(bf16)
        send_ref[half:n, 8:16, :] = head_state(kc_b, vc).reshape(half, 8, 128).astype(bf16)

        lanes = iota((128, 128), 1)

        def packed(latent_total, context_total):
            lh, ll = halves(latent_total)
            ch, cl = halves(context_total)
            lat2 = jnp.where(lanes < 32, lh.astype(f32), ll.astype(f32))
            ctx2 = jnp.where(lanes < 96, ch.astype(f32), cl.astype(f32))
            return jnp.where(lanes < 64, lat2, ctx2).reshape(half, 8, 128).astype(bf16)

        send_ref[0:half, 16:24, :] = packed(total(f_high, f_low), total(cf_high, cf_low))
        send_ref[half:n, 16:24, :] = packed(total(b_high, b_low), total(cb_high, cb_low))


def mixing(h, gathered, decay_weight, decay_bias, shifts, members):
    T = shifts.shape[0]
    rows, width = h.shape
    steps = 8
    depth = width // steps
    whole = lambda *shape: pl.BlockSpec(shape, lambda i: (0,) * len(shape))
    return pl.pallas_call(
        mixing_kernel,
        grid=(steps,),
        in_specs=[
            pl.BlockSpec((rows, depth), lambda i: (0, i)),
            pl.BlockSpec((depth, 256), lambda i: (i, 1)),
            pl.BlockSpec((depth, 256), lambda i: (i, 2)),
            pl.BlockSpec((depth, 128), lambda i: (i, 6)),
            whole(128, 256),
            whole(1, 256),
            whole(T, 256),
        ],
        out_specs=[whole(T, 256), whole(T, 256), whole(members, 24, 128)],
        out_shape=[
            jax.ShapeDtypeStruct((T, 256), f32),
            jax.ShapeDtypeStruct((T, 256), bf16),
            jax.ShapeDtypeStruct((members, 24, 128), bf16),
        ],
        scratch_shapes=[pltpu.VMEM((rows, 640), f32)],
        compiler_params=pltpu.CompilerParams(vmem_limit_bytes=VMEM_LIMIT),
        name="mixing",
    )(h, gathered, gathered, gathered, decay_weight, decay_bias, shifts)


def chain_kernel(in_ref, out_ref):
    n = in_ref.shape[0]
    backward = lax.axis_index("sp") >= n // 2

    def place(i):
        return jnp.where(backward, n - 1 - i, i)

    def decay(at, lane):
        rows = in_ref[at, 16:24, :].astype(f32)
        return rows[:, lane : lane + 1] + rows[:, lane + 32 : lane + 33]

    state = jnp.zeros((8, 128), f32)
    for i in range(n):
        at = place(i)
        state = decay(at, 64) * state + in_ref[at, 8:16, :].astype(f32)
    for i in range(n):
        at = place(i)
        out_ref[at] = state.astype(bf16)
        if i + 1 < n:
            state = decay(at, 0) * state + in_ref[at, 0:8, :].astype(f32)


def chain(received):
    n = received.shape[0]
    return pl.pallas_call(
        chain_kernel,
        out_shape=jax.ShapeDtypeStruct((n, 8, 128), bf16),
        in_specs=[pl.BlockSpec(memory_space=pltpu.VMEM)],
        out_specs=pl.BlockSpec(memory_space=pltpu.VMEM),
        name="chain",
    )(received)


def output_kernel(loc_ref, lift_ref, entry_ref, gain_ref, w_ref, out_ref, normed):
    @pl.when(pl.program_id(0) == 0)
    def _():
        entry = entry_ref[...].astype(f32)
        head = (iota(entry.shape, 0) // DK) % 2
        spread = jnp.concatenate(
            [jnp.where(head == 0, entry, 0.0), jnp.where(head == 1, entry, 0.0)], axis=1
        ).astype(bf16)
        combined = loc_ref[...] + dot(lift_ref[...], spread)
        for g in range(2):
            part = combined[:, g * DV : (g + 1) * DV]
            scaled = part * lax.rsqrt(jnp.mean(part * part, axis=-1, keepdims=True) + eps)
            normed[:, g * DV : (g + 1) * DV] = (
                scaled * gain_ref[:, g * DV : (g + 1) * DV]
            ).astype(bf16)

    w = w_ref[...]
    for j in range(w.shape[0] // 128):
        rows = slice(j * 128, (j + 1) * 128)
        out_ref[0, :, rows] = (
            dot(normed[:, 0:128], w[rows, 0:128]) + dot(normed[:, 128:256], w[rows, 128:256])
        ).astype(bf16)


def output(loc, lift, entry, gain, gathered, pieces):
    T = loc.shape[0]
    width = gathered.shape[0] // pieces
    whole = lambda *shape: pl.BlockSpec(shape, lambda i: (0,) * len(shape))
    return pl.pallas_call(
        output_kernel,
        grid=(pieces,),
        in_specs=[
            whole(T, 256),
            whole(T, 256),
            whole(256, 128),
            whole(1, 256),
            pl.BlockSpec((width, 256), lambda i: (i, 0)),
        ],
        out_specs=pl.BlockSpec((1, T, width), lambda i: (i, 0, 0)),
        out_shape=jax.ShapeDtypeStruct((pieces, T, width), bf16),
        scratch_shapes=[pltpu.VMEM((T, 256), bf16)],
        compiler_params=pltpu.CompilerParams(vmem_limit_bytes=VMEM_LIMIT),
        name="output",
    )(loc, lift, entry, gain, gathered)


def local(
    latent,
    context,
    cond_latent,
    cond_context,
    mod_weight,
    norm_gain,
    w_query,
    w_key,
    w_value,
    w_rank,
    w_decay,
    decay_bias,
    decay_shift,
    out_gain,
    w_out,
):
    T, width = latent.shape
    members = lax.axis_size("sp")
    pieces = lax.axis_size("tp")
    depth = w_query.shape[0]
    own = jnp.concatenate(
        [w_out[:depth], w_out[depth:], w_query, w_key, w_value, w_rank[0], w_rank[1]], axis=1
    )
    gathered = lax.all_gather(own, "sp").reshape(members * depth, own.shape[1])

    silu = jnp.stack([jax.nn.silu(cond_latent), jax.nn.silu(cond_context)]).astype(bf16)
    terms = jnp.einsum("nd,rdc->nrc", silu, mod_weight, preferred_element_type=f32)
    terms = jnp.concatenate([terms[0], terms[1, :2]], axis=0)
    summed_terms = lax.all_gather(terms, "sp").sum(axis=0)
    rows = sent_to_all(summed_terms, "tp")
    modulation = jnp.moveaxis(rows, 0, 1).reshape(rows.shape[1], width)

    extra = 16 - context.shape[0]
    tokens = jnp.concatenate([latent, context, jnp.zeros((extra, width), bf16)], axis=0)
    widened = tokens.astype(f32)
    normalized = widened * lax.rsqrt(jnp.mean(widened * widened, axis=-1, keepdims=True) + eps)
    is_latent = (jnp.arange(T + 16) < T)[:, None]
    scale = jnp.where(is_latent, modulation[1], modulation[4])
    shift = jnp.where(is_latent, modulation[0], modulation[3])
    h = (normalized * norm_gain * (1.0 + scale) + shift).astype(bf16)

    decay_weight = jnp.zeros((128, 256), bf16)
    decay_weight = decay_weight.at[:64, :128].set(w_decay[0]).at[64:, 128:].set(w_decay[1])
    shifts = jnp.repeat(decay_shift, DK, axis=1)
    shifts = jnp.concatenate([shifts, shifts], axis=1)

    loc, lift, send = mixing(
        h, gathered, decay_weight, decay_bias.reshape(1, 256), shifts, members
    )
    received = lax.all_to_all(send, "sp", split_axis=0, concat_axis=0, tiled=True)
    entries = lax.all_to_all(chain(received), "sp", split_axis=0, concat_axis=0, tiled=True)
    parts = output(
        loc, lift, entries.reshape(members * 8, 128), out_gain.reshape(1, 256), gathered, pieces
    )
    parts = lax.all_to_all(parts, "tp", split_axis=0, concat_axis=0, tiled=True)
    summed = parts.astype(f32).sum(axis=0)
    columns = width // pieces
    own_latent = lax.dynamic_slice_in_dim(latent, lax.axis_index("tp") * columns, columns, 1)
    mixed = (own_latent.astype(f32) + summed_terms[2] * summed).astype(bf16)
    return jnp.moveaxis(sent_to_all(mixed, "tp"), 0, 1).reshape(T, width)


def solution(mesh):
    return jax.shard_map(
        local,
        mesh=mesh,
        in_specs=(
            P(("grp", "sp"), None),
            P(("grp", "sp"), None),
            P(("grp", "sp")),
            P(("grp", "sp")),
            P(None, "sp", "tp"),
            P(),
            P("sp", "tp"),
            P("sp", "tp"),
            P("sp", "tp"),
            P(None, "sp", None),
            P(None, None, "tp"),
            P(None, "tp"),
            P(("grp", "sp"), "tp"),
            P("tp"),
            P("tp", "sp"),
        ),
        out_specs=P(("grp", "sp"), None),
        check_vma=False,
    )
```

```python
import jax
import jax.numpy as jnp
from jax import lax
from jax.experimental import pallas as pl
from jax.experimental.pallas import tpu as pltpu
from jax.sharding import PartitionSpec as P

DK = 64
DV = 128
eps = 1e-06
normalizer = 16.0
f32 = jnp.float32
bf16 = jnp.bfloat16
VMEM_LIMIT = 50 * 1024 * 1024


def sent_to_all(array, axis):
    copies = jnp.broadcast_to(array, (lax.axis_size(axis), *array.shape))
    return lax.all_to_all(copies, axis, split_axis=0, concat_axis=0, tiled=True)


def dot(a, b):
    return jnp.dot(a, b, preferred_element_type=f32)


def dot_nt(a, b):
    return lax.dot_general(a, b, (((1,), (1,)), ((), ())), preferred_element_type=f32)


def dot_tn(a, b):
    return lax.dot_general(a, b, (((0,), (0,)), ((), ())), preferred_element_type=f32)


def halves(x):
    high = x.astype(bf16)
    low = (x - high.astype(f32)).astype(bf16)
    return high, low


def iota(shape, dim):
    return lax.broadcasted_iota(jnp.int32, shape, dim)


def log_sigmoid(u):
    return jnp.minimum(u, 0.0) - jnp.log1p(jnp.exp(-jnp.abs(u)))


def head_state(keys, values):
    both = dot_tn(keys, values)
    rows = iota((2 * DK, DV), 0)
    return jnp.where(rows < DK, both[:, :DV], both[:, DV:])


def mixing_kernel(
    h_ref, wqk_ref, wv_ref, wr_ref, wd_ref, bias_ref, shift_ref,
    loc_ref, lift_ref, send_ref, acc,
):
    step = pl.program_id(0)
    T = shift_ref.shape[0]
    C = h_ref.shape[0] - T
    h = h_ref[...]

    @pl.when(step == 0)
    def _():
        acc[...] = jnp.zeros_like(acc)

    acc[:, 0:256] += dot(h, wqk_ref[...])
    acc[:, 256:512] += dot(h, wv_ref[...])
    acc[:, 512:640] += dot(h, wr_ref[...])

    @pl.when(step == pl.num_programs(0) - 1)
    def _():
        q16 = acc[0:T, 0:128].astype(bf16)
        k16 = acc[0:T, 128:256].astype(bf16)
        v = acc[0:T, 256:512].astype(bf16)
        q = q16.astype(f32)
        k = k16.astype(f32)
        ranks = acc[:, 512:640].astype(bf16)
        logs = log_sigmoid(dot(ranks, wd_ref[...]) + bias_ref[...]) / normalizer
        lat = logs[0:T] + shift_ref[...]
        f_high, f_low = halves(lat[:, 0:128])
        b_high, b_low = halves(lat[:, 128:256])
        f_pair = jnp.concatenate([f_high, f_low], axis=1)
        b_pair = jnp.concatenate([b_high, b_low], axis=1)

        def summed(where, pair):
            both = dot(jnp.where(where, 1.0, 0.0).astype(bf16), pair)
            return both[:, 0:128] + both[:, 128:256]

        r = iota((T, T), 0)
        s = iota((T, T), 1)
        lane = iota((T, 128), 1)
        row = iota((T, 128), 0)
        first = lane < DK
        zero = jnp.zeros((T, 128), bf16)

        def scores(qs, ks):
            return (
                dot_nt(qs, jnp.where(first, ks, zero)),
                dot_nt(qs, jnp.where(first, zero, ks)),
            )

        s0, s1 = scores(q16, k16)
        s0 = 2.0 * s0
        s1 = 2.0 * s1
        m = 1
        while m < T:
            base = (r // (2 * m)) * (2 * m)
            ref = base + m
            upper = r >= ref
            lower = r < ref
            d_f = (upper & (s >= ref) & (s <= r)) | (lower & (s > r) & (s < ref))
            d_b = (upper & (s >= ref) & (s < r)) | (lower & (s >= r) & (s < ref))
            fac_f = jnp.exp(summed(d_f, f_pair))
            fac_b = jnp.exp(summed(d_b, b_pair))
            up = (row & m) != 0
            qs = (q * jnp.where(up, fac_f, fac_b)).astype(bf16)
            ks = (k * jnp.where(up, fac_b, fac_f)).astype(bf16)
            m0, m1 = scores(qs, ks)
            pick = ((r ^ s) >= m) & ((r ^ s) < 2 * m)
            s0 = jnp.where(pick, m0, s0)
            s1 = jnp.where(pick, m1, s1)
            m *= 2
        loc_ref[:, 0:128] = dot(s0.astype(bf16), v[:, 0:128])
        loc_ref[:, 128:256] = dot(s1.astype(bf16), v[:, 128:256])

        lift_ref[:, 0:128] = (q * jnp.exp(summed(s <= r, f_pair))).astype(bf16)
        lift_ref[:, 128:256] = (q * jnp.exp(summed(s >= r, b_pair))).astype(bf16)
        k_f = (k * jnp.exp(summed(s > r, f_pair))).astype(bf16)
        k_b = (k * jnp.exp(summed(s < r, b_pair))).astype(bf16)

        def total(high, low):
            ones = jnp.ones((high.shape[0], 128), bf16)
            return jnp.exp(dot_tn(high, ones) + dot_tn(low, ones))

        n = send_ref.shape[0]
        st_f = head_state(k_f, v)
        st_b = head_state(k_b, v)
        half = n // 2
        send_ref[0:half, 0:8, :] = st_f.reshape(half, 8, 128).astype(bf16)
        send_ref[half:n, 0:8, :] = st_b.reshape(half, 8, 128).astype(bf16)

        crow = iota((C, 128), 0)
        live = crow < 8
        kc = jnp.where(live, acc[T : T + C, 128:256].astype(bf16).astype(f32), 0.0)
        vc = acc[T : T + C, 256:512].astype(bf16)
        ctx_f = jnp.where(live, logs[T : T + C, 0:128], 0.0)
        ctx_b = jnp.where(live, logs[T : T + C, 128:256], 0.0)
        cf_high, cf_low = halves(ctx_f)
        cb_high, cb_low = halves(ctx_b)
        rc = iota((C, C), 0)
        sc = iota((C, C), 1)
        kc_f = (kc * jnp.exp(summed(sc > rc, jnp.concatenate([cf_high, cf_low], axis=1)))).astype(bf16)
        kc_b = (kc * jnp.exp(summed(sc < rc, jnp.concatenate([cb_high, cb_low], axis=1)))).astype(bf16)
        send_ref[0:half, 8:16, :] = head_state(kc_f, vc).reshape(half, 8, 128).astype(bf16)
        send_ref[half:n, 8:16, :] = head_state(kc_b, vc).reshape(half, 8, 128).astype(bf16)

        lanes = iota((128, 128), 1)

        def packed(latent_total, context_total):
            lh, ll = halves(latent_total)
            ch, cl = halves(context_total)
            lat2 = jnp.where(lanes < 32, lh.astype(f32), ll.astype(f32))
            ctx2 = jnp.where(lanes < 96, ch.astype(f32), cl.astype(f32))
            return jnp.where(lanes < 64, lat2, ctx2).reshape(half, 8, 128).astype(bf16)

        send_ref[0:half, 16:24, :] = packed(total(f_high, f_low), total(cf_high, cf_low))
        send_ref[half:n, 16:24, :] = packed(total(b_high, b_low), total(cb_high, cb_low))


def mixing(h, gathered, decay_weight, decay_bias, shifts, members):
    T = shifts.shape[0]
    rows, width = h.shape
    steps = 8
    depth = width // steps
    whole = lambda *shape: pl.BlockSpec(shape, lambda i: (0,) * len(shape))
    return pl.pallas_call(
        mixing_kernel,
        grid=(steps,),
        in_specs=[
            pl.BlockSpec((rows, depth), lambda i: (0, i)),
            pl.BlockSpec((depth, 256), lambda i: (i, 1)),
            pl.BlockSpec((depth, 256), lambda i: (i, 2)),
            pl.BlockSpec((depth, 128), lambda i: (i, 6)),
            whole(128, 256),
            whole(1, 256),
            whole(T, 256),
        ],
        out_specs=[whole(T, 256), whole(T, 256), whole(members, 24, 128)],
        out_shape=[
            jax.ShapeDtypeStruct((T, 256), f32),
            jax.ShapeDtypeStruct((T, 256), bf16),
            jax.ShapeDtypeStruct((members, 24, 128), bf16),
        ],
        scratch_shapes=[pltpu.VMEM((rows, 640), f32)],
        compiler_params=pltpu.CompilerParams(vmem_limit_bytes=VMEM_LIMIT),
        name="mixing",
    )(h, gathered, gathered, gathered, decay_weight, decay_bias, shifts)


def chain_kernel(in_ref, out_ref):
    n = in_ref.shape[0]
    backward = lax.axis_index("sp") >= n // 2

    def place(i):
        return jnp.where(backward, n - 1 - i, i)

    def decay(at, lane):
        rows = in_ref[at, 16:24, :].astype(f32)
        return rows[:, lane : lane + 1] + rows[:, lane + 32 : lane + 33]

    state = jnp.zeros((8, 128), f32)
    for i in range(n):
        at = place(i)
        state = decay(at, 64) * state + in_ref[at, 8:16, :].astype(f32)
    for i in range(n):
        at = place(i)
        out_ref[at] = state.astype(bf16)
        if i + 1 < n:
            state = decay(at, 0) * state + in_ref[at, 0:8, :].astype(f32)


def chain(received):
    n = received.shape[0]
    return pl.pallas_call(
        chain_kernel,
        out_shape=jax.ShapeDtypeStruct((n, 8, 128), bf16),
        in_specs=[pl.BlockSpec(memory_space=pltpu.VMEM)],
        out_specs=pl.BlockSpec(memory_space=pltpu.VMEM),
        name="chain",
    )(received)


def normalized_output(loc_ref, lift_ref, entry_ref, gain_ref, normed):
    entry = entry_ref[...].astype(f32)
    head = (iota(entry.shape, 0) // DK) % 2
    spread = jnp.concatenate(
        [jnp.where(head == 0, entry, 0.0), jnp.where(head == 1, entry, 0.0)], axis=1
    ).astype(bf16)
    combined = loc_ref[...] + dot(lift_ref[...], spread)
    for g in range(2):
        part = combined[:, g * DV : (g + 1) * DV]
        scaled = part * lax.rsqrt(jnp.mean(part * part, axis=-1, keepdims=True) + eps)
        normed[:, g * DV : (g + 1) * DV] = (
            scaled * gain_ref[:, g * DV : (g + 1) * DV]
        ).astype(bf16)


def column(normed, w, j):
    rows = slice(j * 128, (j + 1) * 128)
    return dot(normed[:, 0:128], w[rows, 0:128]) + dot(normed[:, 128:256], w[rows, 128:256])


def sent_kernel(order_ref, loc_ref, lift_ref, entry_ref, gain_ref, w_ref, normed, out_ref):
    @pl.when(pl.program_id(0) == 0)
    def _():
        normalized_output(loc_ref, lift_ref, entry_ref, gain_ref, normed)

    w = w_ref[...]
    for j in range(w.shape[0] // 128):
        out_ref[0, :, j * 128 : (j + 1) * 128] = column(normed, w, j).astype(bf16)


def kept_kernel(order_ref, normed, received_ref, w_ref, *out_refs):
    w = w_ref[...]
    for k, out_ref in enumerate(out_refs):

        @pl.when(pl.program_id(0) == k)
        def _():
            for j in range(w.shape[0] // 128):
                cols = slice(j * 128, (j + 1) * 128)
                out_ref[:, cols] = (
                    column(normed, w, j) + received_ref[0, :, cols].astype(f32)
                ).astype(bf16)


def constant_block(*shape):
    return pl.BlockSpec(shape, lambda i, order: (0,) * len(shape))


def sent_parts(order, loc, lift, entry, gain, gathered, width):
    T = loc.shape[0]
    chips = order.shape[0]
    return pl.pallas_call(
        sent_kernel,
        grid_spec=pltpu.PrefetchScalarGridSpec(
            num_scalar_prefetch=1,
            grid=(chips,),
            in_specs=[
                constant_block(T, 256),
                constant_block(T, 256),
                constant_block(256, 128),
                constant_block(1, 256),
                pl.BlockSpec((width, 256), lambda i, order: (order[i], 0)),
            ],
            out_specs=[
                constant_block(T, 256),
                pl.BlockSpec((1, T, width), lambda i, order: (i, 0, 0)),
            ],
        ),
        out_shape=[
            jax.ShapeDtypeStruct((T, 256), bf16),
            jax.ShapeDtypeStruct((chips, T, width), bf16),
        ],
        compiler_params=pltpu.CompilerParams(vmem_limit_bytes=VMEM_LIMIT),
        name="sent",
    )(order, loc, lift, entry, gain, gathered)


def kept_parts(order, normed, received, gathered, width):
    T = normed.shape[0]
    chips = order.shape[0]
    return pl.pallas_call(
        kept_kernel,
        grid_spec=pltpu.PrefetchScalarGridSpec(
            num_scalar_prefetch=1,
            grid=(chips,),
            in_specs=[
                constant_block(T, 256),
                pl.BlockSpec((1, T, width), lambda i, order: (i, 0, 0)),
                pl.BlockSpec((width, 256), lambda i, order: (order[i], 0)),
            ],
            out_specs=[constant_block(T, width)] * chips,
        ),
        out_shape=[jax.ShapeDtypeStruct((T, width), bf16)] * chips,
        compiler_params=pltpu.CompilerParams(vmem_limit_bytes=VMEM_LIMIT),
        name="kept",
    )(order, normed, received, gathered)


def joined_kernel(*refs):
    out_ref = refs[-1]
    pieces = refs[:-1]
    chips = len(pieces) // 2
    place = lax.axis_index("tp")
    width = pieces[0].shape[1]
    for i in range(chips):
        base = 2 * lax.rem(place // 2 + i, chips)
        for piece, core in ((pieces[i], place % 2), (pieces[chips + i], 1 - place % 2)):
            start = pl.multiple_of((base + core) * width, width)
            out_ref[:, pl.ds(start, width)] = piece[...]


def joined(pieces):
    T, width = pieces[0].shape
    vmem = pl.BlockSpec(memory_space=pltpu.VMEM)
    return pl.pallas_call(
        joined_kernel,
        out_shape=jax.ShapeDtypeStruct((T, width * len(pieces)), bf16),
        in_specs=[vmem] * len(pieces),
        out_specs=vmem,
        compiler_params=pltpu.CompilerParams(vmem_limit_bytes=VMEM_LIMIT),
        name="joined",
    )(*pieces)


def to_partner(array):
    n = lax.axis_size("tp")
    return lax.ppermute(array, "tp", [(i, i ^ 1) for i in range(n)])


def to_chip(array, ahead):
    n = lax.axis_size("tp")
    return lax.ppermute(array, "tp", [(i, (i + 2 * ahead) % n) for i in range(n)])


def local(
    latent,
    context,
    cond_latent,
    cond_context,
    mod_weight,
    norm_gain,
    w_query,
    w_key,
    w_value,
    w_rank,
    w_decay,
    decay_bias,
    decay_shift,
    out_gain,
    w_out,
):
    T, width = latent.shape
    members = lax.axis_size("sp")
    pieces = lax.axis_size("tp")
    depth = w_query.shape[0]
    own = jnp.concatenate(
        [w_out[:depth], w_out[depth:], w_query, w_key, w_value, w_rank[0], w_rank[1]], axis=1
    )
    gathered = lax.all_gather(own, "sp").reshape(members * depth, own.shape[1])

    silu = jnp.stack([jax.nn.silu(cond_latent), jax.nn.silu(cond_context)]).astype(bf16)
    terms = jnp.einsum("nd,rdc->nrc", silu, mod_weight, preferred_element_type=f32)
    terms = jnp.concatenate([terms[0], terms[1, :2]], axis=0)
    summed_terms = lax.all_gather(terms, "sp").sum(axis=0)
    rows = sent_to_all(summed_terms, "tp")
    modulation = jnp.moveaxis(rows, 0, 1).reshape(rows.shape[1], width)

    extra = 16 - context.shape[0]
    tokens = jnp.concatenate([latent, context, jnp.zeros((extra, width), bf16)], axis=0)
    widened = tokens.astype(f32)
    normalized = widened * lax.rsqrt(jnp.mean(widened * widened, axis=-1, keepdims=True) + eps)
    is_latent = (jnp.arange(T + 16) < T)[:, None]
    scale = jnp.where(is_latent, modulation[1], modulation[4])
    shift = jnp.where(is_latent, modulation[0], modulation[3])
    h = (normalized * norm_gain * (1.0 + scale) + shift).astype(bf16)

    decay_weight = jnp.zeros((128, 256), bf16)
    decay_weight = decay_weight.at[:64, :128].set(w_decay[0]).at[64:, 128:].set(w_decay[1])
    shifts = jnp.repeat(decay_shift, DK, axis=1)
    shifts = jnp.concatenate([shifts, shifts], axis=1)

    loc, lift, send = mixing(
        h, gathered, decay_weight, decay_bias.reshape(1, 256), shifts, members
    )
    received = lax.all_to_all(send, "sp", split_axis=0, concat_axis=0, tiled=True)
    entries = lax.all_to_all(chain(received), "sp", split_axis=0, concat_axis=0, tiled=True)
    columns = width // pieces
    chips = pieces // 2
    place = lax.axis_index("tp")
    order = 2 * ((place // 2 + jnp.arange(chips)) % chips) + place % 2
    normed, sent = sent_parts(
        order ^ 1, loc, lift, entries.reshape(members * 8, 128), out_gain.reshape(1, 256),
        gathered, columns,
    )
    sums = kept_parts(order, normed, to_partner(sent), gathered, columns)
    own_latent = lax.dynamic_slice_in_dim(latent, place * columns, columns, 1)
    summed = sums[0].astype(f32)
    for i in range(1, chips):
        summed = summed + to_chip(sums[i], i).astype(f32)
    mixed = (own_latent.astype(f32) + summed_terms[2] * summed).astype(bf16)
    mine = [mixed] + [to_chip(mixed, chips - i) for i in range(1, chips)]
    theirs = [to_partner(piece) for piece in mine]
    return joined(mine + theirs)


def solution(mesh):
    return jax.shard_map(
        local,
        mesh=mesh,
        in_specs=(
            P(("grp", "sp"), None),
            P(("grp", "sp"), None),
            P(("grp", "sp")),
            P(("grp", "sp")),
            P(None, "sp", "tp"),
            P(),
            P("sp", "tp"),
            P("sp", "tp"),
            P("sp", "tp"),
            P(None, "sp", None),
            P(None, None, "tp"),
            P(None, "tp"),
            P(("grp", "sp"), "tp"),
            P("tp"),
            P("tp", "sp"),
        ),
        out_specs=P(("grp", "sp"), None),
        check_vma=False,
    )
```

```python
import jax
import jax.numpy as jnp
from jax import lax
from jax.experimental import pallas as pl
from jax.experimental.pallas import tpu as pltpu
from jax.sharding import PartitionSpec as P

DK = 64
DV = 128
eps = 1e-06
normalizer = 16.0
f32 = jnp.float32
bf16 = jnp.bfloat16
f16 = jnp.float16
WEIGHT_SCALE = 2.0**17
TERM_SCALE = 2.0**9
VMEM_LIMIT = 50 * 1024 * 1024


def sent_to_all(array, axis):
    copies = jnp.broadcast_to(array, (lax.axis_size(axis), *array.shape))
    return lax.all_to_all(copies, axis, split_axis=0, concat_axis=0, tiled=True)


def dot(a, b):
    return jnp.dot(a, b, preferred_element_type=f32)


def dot_nt(a, b):
    return lax.dot_general(a, b, (((1,), (1,)), ((), ())), preferred_element_type=f32)


def dot_tn(a, b):
    return lax.dot_general(a, b, (((0,), (0,)), ((), ())), preferred_element_type=f32)


def halves(x):
    high = x.astype(bf16)
    low = (x - high.astype(f32)).astype(bf16)
    return high, low


def iota(shape, dim):
    return lax.broadcasted_iota(jnp.int32, shape, dim)


def log_sigmoid(u):
    return jnp.minimum(u, 0.0) - jnp.log1p(jnp.exp(-jnp.abs(u)))


def head_state(keys, values):
    both = dot_tn(keys, values)
    rows = iota((2 * DK, DV), 0)
    return jnp.where(rows < DK, both[:, :DV], both[:, DV:])


def prepare_kernel(
    cond_l_ref, cond_c_ref, mod_ref, q_ref, k_ref, v_ref, rank_ref, out_w_ref, out_ref
):
    depth = q_ref.shape[0]

    def put(block, array):
        out_ref[block] = array.astype(f32) * WEIGHT_SCALE

    put(0, out_w_ref[0:depth])
    put(1, out_w_ref[depth : 2 * depth])
    put(2, q_ref[...])
    put(3, k_ref[...])
    put(4, v_ref[:, 0:128])
    put(5, v_ref[:, 128:256])
    put(6, rank_ref[...].astype(f32).T)

    def silu(c):
        return c / (1.0 + jnp.exp(-c))

    row = iota((16, depth), 0)
    conds = jnp.where(
        row == 0, silu(cond_l_ref[...]), jnp.where(row == 1, silu(cond_c_ref[...]), 0.0)
    ).astype(bf16)
    out_ref[7] = jnp.zeros((depth, 128), f32)
    terms = [dot(conds, mod_ref[r]) * TERM_SCALE for r in range(3)]
    vectors = [(terms[0], 0), (terms[1], 0), (terms[2], 0), (terms[0], 1), (terms[1], 1)]
    columns = mod_ref.shape[2] // 128
    lines = len(vectors) * columns
    for n, (term, at) in enumerate(vectors):
        for c in range(columns):
            line = term[at : at + 1, c * 128 : (c + 1) * 128]
            high = line.astype(bf16).astype(f32)
            spot = n * columns + c
            out_ref[7, spot : spot + 1, :] = high
            out_ref[7, lines + spot : lines + spot + 1, :] = line - high


def prepare(cond_latent, cond_context, mod_weight, w_query, w_key, w_value, w_rank, w_out):
    depth = w_query.shape[0]
    vmem = pl.BlockSpec(memory_space=pltpu.VMEM)
    ranks = jnp.swapaxes(w_rank, 1, 2).reshape(128, depth)
    return pl.pallas_call(
        prepare_kernel,
        out_shape=jax.ShapeDtypeStruct((8, depth, 128), f32),
        in_specs=[vmem] * 8,
        out_specs=vmem,
        name="prepare",
    )(
        cond_latent.reshape(1, depth), cond_context.reshape(1, depth),
        mod_weight, w_query, w_key, w_value, ranks, w_out,
    )


def stats_kernel(latent_ref, context_ref, out_ref):
    T = latent_ref.shape[0]
    C = context_ref.shape[0]
    for ref, at, size in ((latent_ref, 0, T), (context_ref, T, C)):
        x = ref[...].astype(f32)
        scale = lax.rsqrt(jnp.mean(x * x, axis=-1, keepdims=True) + eps)
        out_ref[at : at + size, :] = jnp.broadcast_to(scale, (size, 128))


def stats(latent, context):
    T, C = latent.shape[0], context.shape[0]
    vmem = pl.BlockSpec(memory_space=pltpu.VMEM)
    return pl.pallas_call(
        stats_kernel,
        out_shape=jax.ShapeDtypeStruct((T + C, 128), f32),
        in_specs=[vmem] * 2,
        out_specs=vmem,
        compiler_params=pltpu.CompilerParams(vmem_limit_bytes=VMEM_LIMIT),
        name="stats",
    )(latent, context)


def mixing_kernel(
    latent_ref, context_ref, stats_ref, rows_ref, gain_ref,
    wq_ref, wk_ref, wv0_ref, wv1_ref, wr_ref, wd_ref, bias_ref, shift_ref,
    loc_ref, lift_ref, send_ref, acc,
):
    step = pl.program_id(0)
    T = latent_ref.shape[0]
    C = context_ref.shape[0]
    columns = rows_ref.shape[1] // 5

    @pl.when(step == 0)
    def _():
        acc[...] = jnp.zeros_like(acc)

    def modulated(ref, at, size, shift_row, scale_row):
        parts = []
        for c in range(columns):
            cols = slice(c * 128, (c + 1) * 128)
            spot = scale_row * columns + c
            scale = gain_ref[0, :, cols] * (1.0 + rows_ref[0, spot : spot + 1, :])
            spot = shift_row * columns + c
            shift = rows_ref[0, spot : spot + 1, :]
            x = ref[:, cols].astype(f32) * stats_ref[at : at + size, :]
            parts.append((x * scale + shift).astype(bf16))
        return jnp.concatenate(parts, axis=1)

    w_qk = jnp.concatenate([wq_ref[0], wk_ref[0]], axis=1)
    w_v = jnp.concatenate([wv0_ref[0], wv1_ref[0]], axis=1)
    h = modulated(latent_ref, 0, T, 0, 1)
    hc = modulated(context_ref, T, C, 3, 4)
    h = jnp.concatenate([h, hc, jnp.zeros((acc.shape[0] - T - C, h.shape[1]), bf16)], axis=0)
    acc[:, 0:256] += dot(h, w_qk)
    acc[:, 256:512] += dot(h, w_v)
    acc[:, 512:640] += dot(h, wr_ref[0])

    @pl.when(step == pl.num_programs(0) - 1)
    def _():
        C = acc.shape[0] - T
        q16 = acc[0:T, 0:128].astype(bf16)
        k16 = acc[0:T, 128:256].astype(bf16)
        v = acc[0:T, 256:512].astype(bf16)
        q = q16.astype(f32)
        k = k16.astype(f32)
        ranks = acc[:, 512:640].astype(bf16)
        rank_lane = iota(ranks.shape, 1)
        none = jnp.zeros_like(ranks)
        pre = jnp.concatenate(
            [
                dot(jnp.where(rank_lane < 64, ranks, none), wd_ref[...]) + bias_ref[0:1, :],
                dot(jnp.where(rank_lane < 64, none, ranks), wd_ref[...]) + bias_ref[1:2, :],
            ],
            axis=1,
        )
        logs = log_sigmoid(pre) / normalizer

        def down(h):
            return jnp.broadcast_to(shift_ref[h : h + 1, :], (128, T)).T

        shifts = jnp.where(iota((T, 128), 1) < DK, down(0), down(1))
        lat = logs[0:T] + jnp.concatenate([shifts, shifts], axis=1)
        f_high, f_low = halves(lat[:, 0:128])
        b_high, b_low = halves(lat[:, 128:256])
        f_pair = jnp.concatenate([f_high, f_low], axis=1)
        b_pair = jnp.concatenate([b_high, b_low], axis=1)

        def summed(where, pair):
            both = dot(jnp.where(where, 1.0, 0.0).astype(bf16), pair)
            return both[:, 0:128] + both[:, 128:256]

        r = iota((T, T), 0)
        s = iota((T, T), 1)
        lane = iota((T, 128), 1)
        row = iota((T, 128), 0)
        first = lane < DK
        zero = jnp.zeros((T, 128), bf16)

        def scores(qs, ks):
            return (
                dot_nt(qs, jnp.where(first, ks, zero)),
                dot_nt(qs, jnp.where(first, zero, ks)),
            )

        s0, s1 = scores(q16, k16)
        s0 = 2.0 * s0
        s1 = 2.0 * s1
        m = 1
        while m < T:
            base = (r // (2 * m)) * (2 * m)
            ref = base + m
            upper = r >= ref
            lower = r < ref
            d_f = (upper & (s >= ref) & (s <= r)) | (lower & (s > r) & (s < ref))
            d_b = (upper & (s >= ref) & (s < r)) | (lower & (s >= r) & (s < ref))
            fac_f = jnp.exp(summed(d_f, f_pair))
            fac_b = jnp.exp(summed(d_b, b_pair))
            up = (row & m) != 0
            qs = (q * jnp.where(up, fac_f, fac_b)).astype(bf16)
            ks = (k * jnp.where(up, fac_b, fac_f)).astype(bf16)
            m0, m1 = scores(qs, ks)
            pick = ((r ^ s) >= m) & ((r ^ s) < 2 * m)
            s0 = jnp.where(pick, m0, s0)
            s1 = jnp.where(pick, m1, s1)
            m *= 2
        loc_ref[:, 0:128] = dot(s0.astype(bf16), v[:, 0:128])
        loc_ref[:, 128:256] = dot(s1.astype(bf16), v[:, 128:256])

        lift_ref[:, 0:128] = (q * jnp.exp(summed(s <= r, f_pair))).astype(bf16)
        lift_ref[:, 128:256] = (q * jnp.exp(summed(s >= r, b_pair))).astype(bf16)
        k_f = (k * jnp.exp(summed(s > r, f_pair))).astype(bf16)
        k_b = (k * jnp.exp(summed(s < r, b_pair))).astype(bf16)

        def total(high, low):
            ones = jnp.ones((high.shape[0], 128), bf16)
            return jnp.exp(dot_tn(high, ones) + dot_tn(low, ones))

        n = send_ref.shape[0]
        st_f = head_state(k_f, v)
        st_b = head_state(k_b, v)
        half = n // 2
        send_ref[0:half, 0:8, :] = st_f.reshape(half, 8, 128).astype(bf16)
        send_ref[half:n, 0:8, :] = st_b.reshape(half, 8, 128).astype(bf16)

        crow = iota((C, 128), 0)
        live = crow < 8
        kc = jnp.where(live, acc[T : T + C, 128:256].astype(bf16).astype(f32), 0.0)
        vc = acc[T : T + C, 256:512].astype(bf16)
        ctx_f = jnp.where(live, logs[T : T + C, 0:128], 0.0)
        ctx_b = jnp.where(live, logs[T : T + C, 128:256], 0.0)
        cf_high, cf_low = halves(ctx_f)
        cb_high, cb_low = halves(ctx_b)
        rc = iota((C, C), 0)
        sc = iota((C, C), 1)
        kc_f = (kc * jnp.exp(summed(sc > rc, jnp.concatenate([cf_high, cf_low], axis=1)))).astype(bf16)
        kc_b = (kc * jnp.exp(summed(sc < rc, jnp.concatenate([cb_high, cb_low], axis=1)))).astype(bf16)
        send_ref[0:half, 8:16, :] = head_state(kc_f, vc).reshape(half, 8, 128).astype(bf16)
        send_ref[half:n, 8:16, :] = head_state(kc_b, vc).reshape(half, 8, 128).astype(bf16)

        lanes = iota((128, 128), 1)

        def packed(latent_total, context_total):
            lh, ll = halves(latent_total)
            ch, cl = halves(context_total)
            lat2 = jnp.where(lanes < 32, lh.astype(f32), ll.astype(f32))
            ctx2 = jnp.where(lanes < 96, ch.astype(f32), cl.astype(f32))
            return jnp.where(lanes < 64, lat2, ctx2).reshape(half, 8, 128).astype(bf16)

        send_ref[0:half, 16:24, :] = packed(total(f_high, f_low), total(cf_high, cf_low))
        send_ref[half:n, 16:24, :] = packed(total(b_high, b_low), total(cb_high, cb_low))


def mixing(
    latent, context, scales, rows, gain, gathered, w_decay, decay_bias, decay_shift, members
):
    T, width = latent.shape
    C = context.shape[0]
    steps = rows.shape[0]
    depth = width // steps
    whole = lambda *shape: pl.BlockSpec(shape, lambda i: (0,) * len(shape))
    return pl.pallas_call(
        mixing_kernel,
        grid=(steps,),
        in_specs=[
            pl.BlockSpec((T, depth), lambda i: (0, i)),
            pl.BlockSpec((C, depth), lambda i: (0, i)),
            whole(T + C, 128),
            pl.BlockSpec((1, *rows.shape[1:]), lambda i: (i, 0, 0)),
            pl.BlockSpec((1, 1, depth), lambda i: (i, 0, 0)),
            *[pl.BlockSpec((1, depth, 128), lambda i, b=b: (b, i, 0)) for b in range(2, 7)],
            whole(128, 128),
            whole(2, 128),
            whole(2, T),
        ],
        out_specs=[whole(T, 256), whole(T, 256), whole(members, 24, 128)],
        out_shape=[
            jax.ShapeDtypeStruct((T, 256), f32),
            jax.ShapeDtypeStruct((T, 256), bf16),
            jax.ShapeDtypeStruct((members, 24, 128), bf16),
        ],
        scratch_shapes=[pltpu.VMEM((T + 16, 640), f32)],
        compiler_params=pltpu.CompilerParams(vmem_limit_bytes=VMEM_LIMIT),
        name="mixing",
    )(
        latent, context, scales, rows, gain.reshape(steps, 1, depth), *[gathered] * 5,
        w_decay.reshape(128, 128), decay_bias, decay_shift.T,
    )


def chain_kernel(in_ref, out_ref):
    n = in_ref.shape[0]
    backward = lax.axis_index("sp") >= n // 2

    def place(i):
        return jnp.where(backward, n - 1 - i, i)

    def decay(at, lane):
        rows = in_ref[at, 16:24, :].astype(f32)
        return rows[:, lane : lane + 1] + rows[:, lane + 32 : lane + 33]

    state = jnp.zeros((8, 128), f32)
    for i in range(n):
        at = place(i)
        state = decay(at, 64) * state + in_ref[at, 8:16, :].astype(f32)
    for i in range(n):
        at = place(i)
        out_ref[at] = state.astype(bf16)
        if i + 1 < n:
            state = decay(at, 0) * state + in_ref[at, 0:8, :].astype(f32)


def chain(received):
    n = received.shape[0]
    return pl.pallas_call(
        chain_kernel,
        out_shape=jax.ShapeDtypeStruct((n, 8, 128), bf16),
        in_specs=[pl.BlockSpec(memory_space=pltpu.VMEM)],
        out_specs=pl.BlockSpec(memory_space=pltpu.VMEM),
        name="chain",
    )(received)


def normalized_output(loc_ref, lift_ref, entry_ref, gain_ref, normed):
    entry = entry_ref[...].astype(f32)
    head = (iota(entry.shape, 0) // DK) % 2
    spread = jnp.concatenate(
        [jnp.where(head == 0, entry, 0.0), jnp.where(head == 1, entry, 0.0)], axis=1
    ).astype(bf16)
    combined = loc_ref[...] + dot(lift_ref[...], spread)
    for g in range(2):
        part = combined[:, g * DV : (g + 1) * DV]
        scaled = part * lax.rsqrt(jnp.mean(part * part, axis=-1, keepdims=True) + eps)
        normed[:, g * DV : (g + 1) * DV] = (
            scaled * gain_ref[:, g * DV : (g + 1) * DV]
        ).astype(bf16)


def column(normed, w, j):
    rows = slice(j * 128, (j + 1) * 128)
    return dot(normed[:, 0:128], w[0, rows]) + dot(normed[:, 128:256], w[1, rows])


def sent_kernel(order_ref, loc_ref, lift_ref, entry_ref, gain_ref, w_ref, normed, out_ref):
    @pl.when(pl.program_id(0) == 0)
    def _():
        normalized_output(loc_ref, lift_ref, entry_ref, gain_ref, normed)

    w = w_ref[...]
    for j in range(w.shape[1] // 128):
        out_ref[0, :, j * 128 : (j + 1) * 128] = column(normed, w, j).astype(bf16)


def kept_kernel(order_ref, normed, received_ref, w_ref, *out_refs):
    w = w_ref[...]
    for k, out_ref in enumerate(out_refs):

        @pl.when(pl.program_id(0) == k)
        def _():
            for j in range(w.shape[1] // 128):
                cols = slice(j * 128, (j + 1) * 128)
                out_ref[:, cols] = (
                    column(normed, w, j) + received_ref[0, :, cols].astype(f32)
                ).astype(bf16)


def constant_block(*shape):
    return pl.BlockSpec(shape, lambda i, order: (0,) * len(shape))


def sent_parts(order, loc, lift, entry, gain, gathered, width):
    T = loc.shape[0]
    chips = order.shape[0]
    return pl.pallas_call(
        sent_kernel,
        grid_spec=pltpu.PrefetchScalarGridSpec(
            num_scalar_prefetch=1,
            grid=(chips,),
            in_specs=[
                constant_block(T, 256),
                constant_block(T, 256),
                constant_block(256, 128),
                constant_block(1, 256),
                pl.BlockSpec((2, width, 128), lambda i, order: (0, order[i], 0)),
            ],
            out_specs=[
                constant_block(T, 256),
                pl.BlockSpec((1, T, width), lambda i, order: (i, 0, 0)),
            ],
        ),
        out_shape=[
            jax.ShapeDtypeStruct((T, 256), bf16),
            jax.ShapeDtypeStruct((chips, T, width), bf16),
        ],
        compiler_params=pltpu.CompilerParams(vmem_limit_bytes=VMEM_LIMIT),
        name="sent",
    )(order, loc, lift, entry, gain, gathered)


def kept_parts(order, normed, received, gathered, width):
    T = normed.shape[0]
    chips = order.shape[0]
    return pl.pallas_call(
        kept_kernel,
        grid_spec=pltpu.PrefetchScalarGridSpec(
            num_scalar_prefetch=1,
            grid=(chips,),
            in_specs=[
                constant_block(T, 256),
                pl.BlockSpec((1, T, width), lambda i, order: (i, 0, 0)),
                pl.BlockSpec((2, width, 128), lambda i, order: (0, order[i], 0)),
            ],
            out_specs=[constant_block(T, width)] * chips,
        ),
        out_shape=[jax.ShapeDtypeStruct((T, width), bf16)] * chips,
        compiler_params=pltpu.CompilerParams(vmem_limit_bytes=VMEM_LIMIT),
        name="kept",
    )(order, normed, received, gathered)


def joined_kernel(*refs):
    out_ref = refs[-1]
    pieces = refs[:-1]
    chips = len(pieces) // 2
    place = lax.axis_index("tp")
    width = pieces[0].shape[1]
    for i in range(chips):
        base = 2 * lax.rem(place // 2 + i, chips)
        for piece, core in ((pieces[i], place % 2), (pieces[chips + i], 1 - place % 2)):
            start = pl.multiple_of((base + core) * width, width)
            out_ref[:, pl.ds(start, width)] = piece[...]


def joined(pieces):
    T, width = pieces[0].shape
    vmem = pl.BlockSpec(memory_space=pltpu.VMEM)
    return pl.pallas_call(
        joined_kernel,
        out_shape=jax.ShapeDtypeStruct((T, width * len(pieces)), bf16),
        in_specs=[vmem] * len(pieces),
        out_specs=vmem,
        compiler_params=pltpu.CompilerParams(vmem_limit_bytes=VMEM_LIMIT),
        name="joined",
    )(*pieces)


def to_partner(array):
    n = lax.axis_size("tp")
    return lax.ppermute(array, "tp", [(i, i ^ 1) for i in range(n)])


def to_chip(array, ahead):
    n = lax.axis_size("tp")
    return lax.ppermute(array, "tp", [(i, (i + 2 * ahead) % n) for i in range(n)])


def local(
    latent,
    context,
    cond_latent,
    cond_context,
    mod_weight,
    norm_gain,
    w_query,
    w_key,
    w_value,
    w_rank,
    w_decay,
    decay_bias,
    decay_shift,
    out_gain,
    w_out,
):
    T, width = latent.shape
    members = lax.axis_size("sp")
    pieces = lax.axis_size("tp")
    depth = w_query.shape[0]
    own = prepare(
        cond_latent, cond_context, mod_weight, w_query, w_key, w_value, w_rank, w_out
    ).astype(f16)
    everyone = lax.all_gather(own, "sp", axis=1, tiled=True)

    gathered = (everyone[:7].astype(f32) * (1.0 / WEIGHT_SCALE)).astype(bf16)
    lines = 5 * mod_weight.shape[2] // 128
    sums = everyone[7].reshape(members, depth, 128)[:, : 2 * lines].astype(f32).sum(axis=0)
    summed_terms = (sums[:lines] + sums[lines:]) * (1.0 / TERM_SCALE)
    rows = sent_to_all(summed_terms, "tp")
    gate = summed_terms.reshape(5, -1)[2]

    loc, lift, send = mixing(
        latent, context, stats(latent, context), rows, norm_gain, gathered, w_decay, decay_bias,
        decay_shift, members,
    )
    received = lax.all_to_all(send, "sp", split_axis=0, concat_axis=0, tiled=True)
    entries = lax.all_to_all(chain(received), "sp", split_axis=0, concat_axis=0, tiled=True)
    columns = width // pieces
    chips = pieces // 2
    place = lax.axis_index("tp")
    order = 2 * ((place // 2 + jnp.arange(chips)) % chips) + place % 2
    normed, sent = sent_parts(
        order ^ 1, loc, lift, entries.reshape(members * 8, 128), out_gain.reshape(1, 256),
        gathered, columns,
    )
    sums = kept_parts(order, normed, to_partner(sent), gathered, columns)
    own_latent = lax.dynamic_slice_in_dim(latent, place * columns, columns, 1)
    summed = sums[0].astype(f32)
    for i in range(1, chips):
        summed = summed + to_chip(sums[i], i).astype(f32)
    mixed = (own_latent.astype(f32) + gate * summed).astype(bf16)
    mine = [mixed] + [to_chip(mixed, chips - i) for i in range(1, chips)]
    theirs = [to_partner(piece) for piece in mine]
    return joined(mine + theirs)


def solution(mesh):
    return jax.shard_map(
        local,
        mesh=mesh,
        in_specs=(
            P(("grp", "sp"), None),
            P(("grp", "sp"), None),
            P(("grp", "sp")),
            P(("grp", "sp")),
            P(None, "sp", "tp"),
            P(),
            P("sp", "tp"),
            P("sp", "tp"),
            P("sp", "tp"),
            P(None, "sp", None),
            P(None, None, "tp"),
            P(None, "tp"),
            P(("grp", "sp"), "tp"),
            P("tp"),
            P("tp", "sp"),
        ),
        out_specs=P(("grp", "sp"), None),
        check_vma=False,
    )
```

```python
import jax
import jax.numpy as jnp
from jax import lax
from jax.experimental import pallas as pl
from jax.experimental.pallas import tpu as pltpu
from jax.sharding import PartitionSpec as P

DK = 64
DV = 128
eps = 1e-06
normalizer = 16.0
f32 = jnp.float32
bf16 = jnp.bfloat16
f16 = jnp.float16
WEIGHT_SCALE = 2.0**17
TERM_SCALE = 2.0**9
TERM_ROWS = 8
VMEM_LIMIT = 50 * 1024 * 1024


def sent_to_all(array, axis):
    copies = jnp.broadcast_to(array, (lax.axis_size(axis), *array.shape))
    return lax.all_to_all(copies, axis, split_axis=0, concat_axis=0, tiled=True)


def dot(a, b):
    return jnp.dot(a, b, preferred_element_type=f32)


def dot_nt(a, b):
    return lax.dot_general(a, b, (((1,), (1,)), ((), ())), preferred_element_type=f32)


def dot_tn(a, b):
    return lax.dot_general(a, b, (((0,), (0,)), ((), ())), preferred_element_type=f32)


def halves(x):
    high = x.astype(bf16)
    low = (x - high.astype(f32)).astype(bf16)
    return high, low


def iota(shape, dim):
    return lax.broadcasted_iota(jnp.int32, shape, dim)


def log_sigmoid(u):
    return jnp.minimum(u, 0.0) - jnp.log1p(jnp.exp(-jnp.abs(u)))


def head_state(keys, values):
    both = dot_tn(keys, values)
    rows = iota((2 * DK, DV), 0)
    return jnp.where(rows < DK, both[:, :DV], both[:, DV:])


def summed(where, pair):
    both = dot(jnp.where(where, 1.0, 0.0).astype(bf16), pair)
    return both[:, 0:128] + both[:, 128:256]


def prepare_kernel(
    cond_l_ref, cond_c_ref, mod_ref, q_ref, k_ref, v_ref, rank_ref, out_w_ref, out_ref
):
    depth = q_ref.shape[0]

    def put(block, array):
        out_ref[block, 0:depth, :] = array.astype(f32) * WEIGHT_SCALE

    put(0, out_w_ref[0:depth])
    put(1, out_w_ref[depth : 2 * depth])
    put(2, q_ref[...])
    put(3, k_ref[...])
    put(4, v_ref[:, 0:128])
    put(5, v_ref[:, 128:256])
    put(6, rank_ref[...].astype(f32).T)

    def silu(c):
        return c / (1.0 + jnp.exp(-c))

    row = iota((16, depth), 0)
    conds = jnp.where(
        row == 0, silu(cond_l_ref[...]), jnp.where(row == 1, silu(cond_c_ref[...]), 0.0)
    ).astype(bf16)
    blocks = out_ref.shape[0]
    out_ref[:, depth:, :] = jnp.zeros((blocks, TERM_ROWS, 128), f32)
    terms = [dot(conds, mod_ref[r]) * TERM_SCALE for r in range(3)]
    vectors = [(terms[0], 0), (terms[1], 0), (terms[2], 0), (terms[0], 1), (terms[1], 1)]
    columns = mod_ref.shape[2] // 128
    lines = len(vectors) * columns
    for n, (term, at) in enumerate(vectors):
        for c in range(columns):
            line = term[at : at + 1, c * 128 : (c + 1) * 128]
            high = line.astype(bf16).astype(f32)
            spot = n * columns + c
            for at_row, value in ((spot, high), (lines + spot, line - high)):
                place = depth + at_row % TERM_ROWS
                out_ref[at_row // TERM_ROWS, place : place + 1, :] = value


def prepare(cond_latent, cond_context, mod_weight, w_query, w_key, w_value, w_rank, w_out):
    depth = w_query.shape[0]
    vmem = pl.BlockSpec(memory_space=pltpu.VMEM)
    ranks = jnp.swapaxes(w_rank, 1, 2).reshape(128, depth)
    return pl.pallas_call(
        prepare_kernel,
        out_shape=jax.ShapeDtypeStruct((7, depth + TERM_ROWS, 128), f32),
        in_specs=[vmem] * 8,
        out_specs=vmem,
        name="prepare",
    )(
        cond_latent.reshape(1, depth), cond_context.reshape(1, depth),
        mod_weight, w_query, w_key, w_value, ranks, w_out,
    )


def stats_kernel(latent_ref, context_ref, out_ref):
    T = latent_ref.shape[0]
    C = context_ref.shape[0]
    for ref, at, size in ((latent_ref, 0, T), (context_ref, T, C)):
        x = ref[...].astype(f32)
        scale = lax.rsqrt(jnp.mean(x * x, axis=-1, keepdims=True) + eps)
        out_ref[at : at + size, :] = jnp.broadcast_to(scale, (size, 128))


def stats(latent, context):
    T, C = latent.shape[0], context.shape[0]
    vmem = pl.BlockSpec(memory_space=pltpu.VMEM)
    return pl.pallas_call(
        stats_kernel,
        out_shape=jax.ShapeDtypeStruct((T + C, 128), f32),
        in_specs=[vmem] * 2,
        out_specs=vmem,
        compiler_params=pltpu.CompilerParams(vmem_limit_bytes=VMEM_LIMIT),
        name="stats",
    )(latent, context)


def mixing_kernel(
    latent_ref, context_ref, stats_ref, rows_ref, gain_ref,
    wq_ref, wk_ref, wv0_ref, wv1_ref, wr_ref, wd_ref, bias_ref, shift_ref,
    qkv_ref, pairs_ref, send_ref, acc,
):
    step = pl.program_id(0)
    T = latent_ref.shape[0]
    C = context_ref.shape[0]
    columns = rows_ref.shape[1] // 5

    @pl.when(step == 0)
    def _():
        acc[...] = jnp.zeros_like(acc)

    def modulated(ref, at, size, shift_row, scale_row):
        parts = []
        for c in range(columns):
            cols = slice(c * 128, (c + 1) * 128)
            spot = scale_row * columns + c
            scale = gain_ref[0, :, cols] * (1.0 + rows_ref[0, spot : spot + 1, :])
            spot = shift_row * columns + c
            shift = rows_ref[0, spot : spot + 1, :]
            x = ref[:, cols].astype(f32) * stats_ref[at : at + size, :]
            parts.append((x * scale + shift).astype(bf16))
        return jnp.concatenate(parts, axis=1)

    def weight(ref):
        depth = ref.shape[2] - TERM_ROWS
        return jnp.concatenate([ref[0, j, 0:depth] for j in range(ref.shape[1])], axis=0)

    w_qk = jnp.concatenate([weight(wq_ref), weight(wk_ref)], axis=1)
    w_v = jnp.concatenate([weight(wv0_ref), weight(wv1_ref)], axis=1)
    h = modulated(latent_ref, 0, T, 0, 1)
    hc = modulated(context_ref, T, C, 3, 4)
    h = jnp.concatenate([h, hc, jnp.zeros((acc.shape[0] - T - C, h.shape[1]), bf16)], axis=0)
    acc[:, 0:256] += dot(h, w_qk)
    acc[:, 256:512] += dot(h, w_v)
    acc[:, 512:640] += dot(h, weight(wr_ref))

    @pl.when(step == pl.num_programs(0) - 1)
    def _():
        C = acc.shape[0] - T
        unscale = 1.0 / WEIGHT_SCALE
        q16 = (acc[0:T, 0:128] * unscale).astype(bf16)
        k16 = (acc[0:T, 128:256] * unscale).astype(bf16)
        v = (acc[0:T, 256:512] * unscale).astype(bf16)
        k = k16.astype(f32)
        ranks = (acc[:, 512:640] * unscale).astype(bf16)
        rank_lane = iota(ranks.shape, 1)
        none = jnp.zeros_like(ranks)
        pre = jnp.concatenate(
            [
                dot(jnp.where(rank_lane < 64, ranks, none), wd_ref[...]) + bias_ref[0:1, :],
                dot(jnp.where(rank_lane < 64, none, ranks), wd_ref[...]) + bias_ref[1:2, :],
            ],
            axis=1,
        )
        logs = log_sigmoid(pre) / normalizer

        def down(h):
            return jnp.broadcast_to(shift_ref[h : h + 1, :], (128, T)).T

        shifts = jnp.where(iota((T, 128), 1) < DK, down(0), down(1))
        lat = logs[0:T] + jnp.concatenate([shifts, shifts], axis=1)
        qkv_ref[:, 0:128] = q16
        qkv_ref[:, 128:256] = k16
        qkv_ref[:, 256:512] = v
        f_high, f_low = halves(lat[:, 0:128])
        b_high, b_low = halves(lat[:, 128:256])
        f_pair = jnp.concatenate([f_high, f_low], axis=1)
        b_pair = jnp.concatenate([b_high, b_low], axis=1)
        pairs_ref[:, 0:256] = f_pair
        pairs_ref[:, 256:512] = b_pair
        r = iota((T, T), 0)
        s = iota((T, T), 1)
        k_f = (k * jnp.exp(summed(s > r, f_pair))).astype(bf16)
        k_b = (k * jnp.exp(summed(s < r, b_pair))).astype(bf16)

        def total(high, low):
            ones = jnp.ones((high.shape[0], 128), bf16)
            return jnp.exp(dot_tn(high, ones) + dot_tn(low, ones))

        n = send_ref.shape[0]
        st_f = head_state(k_f, v)
        st_b = head_state(k_b, v)
        half = n // 2
        send_ref[0:half, 0:8, :] = st_f.reshape(half, 8, 128).astype(bf16)
        send_ref[half:n, 0:8, :] = st_b.reshape(half, 8, 128).astype(bf16)

        crow = iota((C, 128), 0)
        live = crow < 8
        kc = jnp.where(live, (acc[T : T + C, 128:256] * unscale).astype(bf16).astype(f32), 0.0)
        vc = (acc[T : T + C, 256:512] * unscale).astype(bf16)
        ctx_f = jnp.where(live, logs[T : T + C, 0:128], 0.0)
        ctx_b = jnp.where(live, logs[T : T + C, 128:256], 0.0)
        cf_high, cf_low = halves(ctx_f)
        cb_high, cb_low = halves(ctx_b)
        rc = iota((C, C), 0)
        sc = iota((C, C), 1)
        kc_f = (kc * jnp.exp(summed(sc > rc, jnp.concatenate([cf_high, cf_low], axis=1)))).astype(bf16)
        kc_b = (kc * jnp.exp(summed(sc < rc, jnp.concatenate([cb_high, cb_low], axis=1)))).astype(bf16)
        send_ref[0:half, 8:16, :] = head_state(kc_f, vc).reshape(half, 8, 128).astype(bf16)
        send_ref[half:n, 8:16, :] = head_state(kc_b, vc).reshape(half, 8, 128).astype(bf16)

        lanes = iota((128, 128), 1)

        def packed(latent_total, context_total):
            lh, ll = halves(latent_total)
            ch, cl = halves(context_total)
            lat2 = jnp.where(lanes < 32, lh.astype(f32), ll.astype(f32))
            ctx2 = jnp.where(lanes < 96, ch.astype(f32), cl.astype(f32))
            return jnp.where(lanes < 64, lat2, ctx2).reshape(half, 8, 128).astype(bf16)

        send_ref[0:half, 16:24, :] = packed(total(f_high, f_low), total(cf_high, cf_low))
        send_ref[half:n, 16:24, :] = packed(total(b_high, b_low), total(cb_high, cb_low))


def mixing(
    latent, context, scales, rows, gain, gathered, w_decay, decay_bias, decay_shift, members
):
    T, width = latent.shape
    C = context.shape[0]
    steps = rows.shape[0]
    depth = width // steps
    whole = lambda *shape: pl.BlockSpec(shape, lambda i: (0,) * len(shape))
    return pl.pallas_call(
        mixing_kernel,
        grid=(steps,),
        in_specs=[
            pl.BlockSpec((T, depth), lambda i: (0, i)),
            pl.BlockSpec((C, depth), lambda i: (0, i)),
            whole(T + C, 128),
            pl.BlockSpec((1, *rows.shape[1:]), lambda i: (i, 0, 0)),
            pl.BlockSpec((1, 1, depth), lambda i: (i, 0, 0)),
            *[
                pl.BlockSpec(
                    (1, gathered.shape[1] // steps, gathered.shape[2], 128),
                    lambda i, b=b: (b, i, 0, 0),
                )
                for b in range(2, 7)
            ],
            whole(128, 128),
            whole(2, 128),
            whole(2, T),
        ],
        out_specs=[whole(T, 512), whole(T, 512), whole(members, 24, 128)],
        out_shape=[
            jax.ShapeDtypeStruct((T, 512), bf16),
            jax.ShapeDtypeStruct((T, 512), bf16),
            jax.ShapeDtypeStruct((members, 24, 128), bf16),
        ],
        scratch_shapes=[pltpu.VMEM((T + 16, 640), f32)],
        compiler_params=pltpu.CompilerParams(vmem_limit_bytes=VMEM_LIMIT),
        name="mixing",
    )(
        latent, context, scales, rows, gain.reshape(steps, 1, depth), *[gathered] * 5,
        w_decay.reshape(128, 128), decay_bias, decay_shift.T,
    )


def scores_kernel(qkv_ref, pairs_ref, loc_ref, lift_ref):
    T = qkv_ref.shape[0]
    q16 = qkv_ref[:, 0:128]
    k16 = qkv_ref[:, 128:256]
    v = qkv_ref[:, 256:512]
    q = q16.astype(f32)
    k = k16.astype(f32)
    f_pair = pairs_ref[:, 0:256]
    b_pair = pairs_ref[:, 256:512]
    r = iota((T, T), 0)
    s = iota((T, T), 1)
    lane = iota((T, 128), 1)
    row = iota((T, 128), 0)
    first = lane < DK
    zero = jnp.zeros((T, 128), bf16)

    def scores(qs, ks):
        return (
            dot_nt(qs, jnp.where(first, ks, zero)),
            dot_nt(qs, jnp.where(first, zero, ks)),
        )

    s0, s1 = scores(q16, k16)
    s0 = 2.0 * s0
    s1 = 2.0 * s1
    m = 1
    while m < T:
        base = (r // (2 * m)) * (2 * m)
        ref = base + m
        upper = r >= ref
        lower = r < ref
        d_f = (upper & (s >= ref) & (s <= r)) | (lower & (s > r) & (s < ref))
        d_b = (upper & (s >= ref) & (s < r)) | (lower & (s >= r) & (s < ref))
        fac_f = jnp.exp(summed(d_f, f_pair))
        fac_b = jnp.exp(summed(d_b, b_pair))
        up = (row & m) != 0
        qs = (q * jnp.where(up, fac_f, fac_b)).astype(bf16)
        ks = (k * jnp.where(up, fac_b, fac_f)).astype(bf16)
        m0, m1 = scores(qs, ks)
        pick = ((r ^ s) >= m) & ((r ^ s) < 2 * m)
        s0 = jnp.where(pick, m0, s0)
        s1 = jnp.where(pick, m1, s1)
        m *= 2
    loc_ref[:, 0:128] = dot(s0.astype(bf16), v[:, 0:128])
    loc_ref[:, 128:256] = dot(s1.astype(bf16), v[:, 128:256])
    lift_ref[:, 0:128] = (q * jnp.exp(summed(s <= r, f_pair))).astype(bf16)
    lift_ref[:, 128:256] = (q * jnp.exp(summed(s >= r, b_pair))).astype(bf16)


def local_scores(qkv, pairs):
    T = qkv.shape[0]
    vmem = pl.BlockSpec(memory_space=pltpu.VMEM)
    return pl.pallas_call(
        scores_kernel,
        out_shape=[
            jax.ShapeDtypeStruct((T, 256), f32),
            jax.ShapeDtypeStruct((T, 256), bf16),
        ],
        in_specs=[vmem] * 2,
        out_specs=[vmem] * 2,
        compiler_params=pltpu.CompilerParams(vmem_limit_bytes=VMEM_LIMIT),
        cost_estimate=pl.CostEstimate(
            flops=40 * 2 * T * T * 256, bytes_accessed=T * 4096, transcendentals=20 * T * 128
        ),
        name="scores",
    )(qkv, pairs)


def chain_kernel(in_ref, out_ref):
    n = in_ref.shape[0]
    backward = lax.axis_index("sp") >= n // 2

    def place(i):
        return jnp.where(backward, n - 1 - i, i)

    def decay(at, lane):
        rows = in_ref[at, 16:24, :].astype(f32)
        return rows[:, lane : lane + 1] + rows[:, lane + 32 : lane + 33]

    state = jnp.zeros((8, 128), f32)
    for i in range(n):
        at = place(i)
        state = decay(at, 64) * state + in_ref[at, 8:16, :].astype(f32)
    for i in range(n):
        at = place(i)
        out_ref[at] = state.astype(bf16)
        if i + 1 < n:
            state = decay(at, 0) * state + in_ref[at, 0:8, :].astype(f32)


def chain(received):
    n = received.shape[0]
    return pl.pallas_call(
        chain_kernel,
        out_shape=jax.ShapeDtypeStruct((n, 8, 128), bf16),
        in_specs=[pl.BlockSpec(memory_space=pltpu.VMEM)],
        out_specs=pl.BlockSpec(memory_space=pltpu.VMEM),
        name="chain",
    )(received)


def normalized_output(loc_ref, lift_ref, entry_ref, gain_ref, normed):
    entry = entry_ref[...].astype(f32)
    head = (iota(entry.shape, 0) // DK) % 2
    spread = jnp.concatenate(
        [jnp.where(head == 0, entry, 0.0), jnp.where(head == 1, entry, 0.0)], axis=1
    ).astype(bf16)
    combined = loc_ref[...] + dot(lift_ref[...], spread)
    for g in range(2):
        part = combined[:, g * DV : (g + 1) * DV]
        scaled = part * lax.rsqrt(jnp.mean(part * part, axis=-1, keepdims=True) + eps)
        normed[:, g * DV : (g + 1) * DV] = (
            scaled * gain_ref[:, g * DV : (g + 1) * DV]
        ).astype(bf16)


def column(normed, w, j):
    return (dot(normed[:, 0:128], w[0, j, 0:128]) + dot(normed[:, 128:256], w[1, j, 0:128])) * (1.0 / WEIGHT_SCALE)


def sent_kernel(order_ref, loc_ref, lift_ref, entry_ref, gain_ref, w_ref, normed, out_ref):
    @pl.when(pl.program_id(0) == 0)
    def _():
        normalized_output(loc_ref, lift_ref, entry_ref, gain_ref, normed)

    w = w_ref[...]
    for j in range(w.shape[1]):
        out_ref[0, :, j * 128 : (j + 1) * 128] = column(normed, w, j).astype(bf16)


def kept_kernel(order_ref, normed, received_ref, w_ref, *out_refs):
    w = w_ref[...]
    for k, out_ref in enumerate(out_refs):

        @pl.when(pl.program_id(0) == k)
        def _():
            for j in range(w.shape[1]):
                cols = slice(j * 128, (j + 1) * 128)
                out_ref[:, cols] = (
                    column(normed, w, j) + received_ref[0, :, cols].astype(f32)
                ).astype(bf16)


def constant_block(*shape):
    return pl.BlockSpec(shape, lambda i, order: (0,) * len(shape))


def sent_parts(order, loc, lift, entry, gain, gathered, width):
    T = loc.shape[0]
    chips = order.shape[0]
    return pl.pallas_call(
        sent_kernel,
        grid_spec=pltpu.PrefetchScalarGridSpec(
            num_scalar_prefetch=1,
            grid=(chips,),
            in_specs=[
                constant_block(T, 256),
                constant_block(T, 256),
                constant_block(256, 128),
                constant_block(1, 256),
                pl.BlockSpec(
                    (2, width // 128, gathered.shape[2], 128),
                    lambda i, order: (0, order[i], 0, 0),
                ),
            ],
            out_specs=[
                constant_block(T, 256),
                pl.BlockSpec((1, T, width), lambda i, order: (i, 0, 0)),
            ],
        ),
        out_shape=[
            jax.ShapeDtypeStruct((T, 256), bf16),
            jax.ShapeDtypeStruct((chips, T, width), bf16),
        ],
        compiler_params=pltpu.CompilerParams(vmem_limit_bytes=VMEM_LIMIT),
        name="sent",
    )(order, loc, lift, entry, gain, gathered)


def kept_parts(order, normed, received, gathered, width):
    T = normed.shape[0]
    chips = order.shape[0]
    return pl.pallas_call(
        kept_kernel,
        grid_spec=pltpu.PrefetchScalarGridSpec(
            num_scalar_prefetch=1,
            grid=(chips,),
            in_specs=[
                constant_block(T, 256),
                pl.BlockSpec((1, T, width), lambda i, order: (i, 0, 0)),
                pl.BlockSpec(
                    (2, width // 128, gathered.shape[2], 128),
                    lambda i, order: (0, order[i], 0, 0),
                ),
            ],
            out_specs=[constant_block(T, width)] * chips,
        ),
        out_shape=[jax.ShapeDtypeStruct((T, width), bf16)] * chips,
        compiler_params=pltpu.CompilerParams(vmem_limit_bytes=VMEM_LIMIT),
        name="kept",
    )(order, normed, received, gathered)


def joined_kernel(*refs):
    out_ref = refs[-1]
    pieces = refs[:-1]
    chips = len(pieces) // 2
    place = lax.axis_index("tp")
    width = pieces[0].shape[1]
    for i in range(chips):
        base = 2 * lax.rem(place // 2 + i, chips)
        for piece, core in ((pieces[i], place % 2), (pieces[chips + i], 1 - place % 2)):
            start = pl.multiple_of((base + core) * width, width)
            out_ref[:, pl.ds(start, width)] = piece[...]


def joined(pieces):
    T, width = pieces[0].shape
    vmem = pl.BlockSpec(memory_space=pltpu.VMEM)
    return pl.pallas_call(
        joined_kernel,
        out_shape=jax.ShapeDtypeStruct((T, width * len(pieces)), bf16),
        in_specs=[vmem] * len(pieces),
        out_specs=vmem,
        compiler_params=pltpu.CompilerParams(vmem_limit_bytes=VMEM_LIMIT),
        name="joined",
    )(*pieces)


def to_partner(array):
    n = lax.axis_size("tp")
    return lax.ppermute(array, "tp", [(i, i ^ 1) for i in range(n)])


def to_chip(array, ahead):
    n = lax.axis_size("tp")
    return lax.ppermute(array, "tp", [(i, (i + 2 * ahead) % n) for i in range(n)])


def local(
    latent,
    context,
    cond_latent,
    cond_context,
    mod_weight,
    norm_gain,
    w_query,
    w_key,
    w_value,
    w_rank,
    w_decay,
    decay_bias,
    decay_shift,
    out_gain,
    w_out,
):
    T, width = latent.shape
    members = lax.axis_size("sp")
    pieces = lax.axis_size("tp")
    depth = w_query.shape[0]
    own = prepare(
        cond_latent, cond_context, mod_weight, w_query, w_key, w_value, w_rank, w_out
    ).astype(f16)
    everyone = lax.all_gather(own, "sp", axis=1, tiled=True).astype(bf16)
    gathered = everyone.reshape(own.shape[0], members, depth + TERM_ROWS, 128)
    lines = 5 * mod_weight.shape[2] // 128
    sums = gathered[:, :, depth:].astype(f32).sum(axis=1).reshape(-1, 128)
    summed_terms = (sums[:lines] + sums[lines : 2 * lines]) * (1.0 / TERM_SCALE)
    rows = sent_to_all(summed_terms, "tp")
    gate = summed_terms.reshape(5, -1)[2]

    qkv, pairs, send = mixing(
        latent, context, stats(latent, context), rows, norm_gain, gathered, w_decay, decay_bias,
        decay_shift, members,
    )
    loc, lift = local_scores(qkv, pairs)
    received = lax.all_to_all(send, "sp", split_axis=0, concat_axis=0, tiled=True)
    entries = lax.all_to_all(chain(received), "sp", split_axis=0, concat_axis=0, tiled=True)
    columns = width // pieces
    chips = pieces // 2
    place = lax.axis_index("tp")
    order = 2 * ((place // 2 + jnp.arange(chips)) % chips) + place % 2
    normed, sent = sent_parts(
        order ^ 1, loc, lift, entries.reshape(members * 8, 128), out_gain.reshape(1, 256),
        gathered, columns,
    )
    sums = kept_parts(order, normed, to_partner(sent), gathered, columns)
    own_latent = lax.dynamic_slice_in_dim(latent, place * columns, columns, 1)
    summed = sums[0].astype(f32)
    for i in range(1, chips):
        summed = summed + to_chip(sums[i], i).astype(f32)
    mixed = (own_latent.astype(f32) + gate * summed).astype(bf16)
    mine = [mixed] + [to_chip(mixed, chips - i) for i in range(1, chips)]
    theirs = [to_partner(piece) for piece in mine]
    return joined(mine + theirs)


def solution(mesh):
    return jax.shard_map(
        local,
        mesh=mesh,
        in_specs=(
            P(("grp", "sp"), None),
            P(("grp", "sp"), None),
            P(("grp", "sp")),
            P(("grp", "sp")),
            P(None, "sp", "tp"),
            P(),
            P("sp", "tp"),
            P("sp", "tp"),
            P("sp", "tp"),
            P(None, "sp", None),
            P(None, None, "tp"),
            P(None, "tp"),
            P(("grp", "sp"), "tp"),
            P("tp"),
            P("tp", "sp"),
        ),
        out_specs=P(("grp", "sp"), None),
        check_vma=False,
    )
```

```python
import jax
import jax.numpy as jnp
from jax import lax
from jax.experimental import pallas as pl
from jax.experimental.pallas import tpu as pltpu
from jax.sharding import PartitionSpec as P

DK = 64
DV = 128
eps = 1e-06
normalizer = 16.0
f32 = jnp.float32
bf16 = jnp.bfloat16
f16 = jnp.float16
WEIGHT_SCALE = 2.0**17
TERM_SCALE = 2.0**9
CUTS = 4
OUT_ROWS = 64
TERM_ROWS = 16
HEAD_ROWS = 160
PART = 80
NEAR = 8
VMEM_LIMIT = 50 * 1024 * 1024


def sent_to_all(array, axis):
    copies = jnp.broadcast_to(array, (lax.axis_size(axis), *array.shape))
    return lax.all_to_all(copies, axis, split_axis=0, concat_axis=0, tiled=True)


def dot(a, b):
    return jnp.dot(a, b, preferred_element_type=f32)


def dot_nt(a, b):
    return lax.dot_general(a, b, (((1,), (1,)), ((), ())), preferred_element_type=f32)


def dot_tn(a, b):
    return lax.dot_general(a, b, (((0,), (0,)), ((), ())), preferred_element_type=f32)


def halves(x):
    high = x.astype(bf16)
    low = (x - high.astype(f32)).astype(bf16)
    return high, low


def iota(shape, dim):
    return lax.broadcasted_iota(jnp.int32, shape, dim)


def log_sigmoid(u):
    return jnp.minimum(u, 0.0) - jnp.log1p(jnp.exp(-jnp.abs(u)))


def head_state(keys, values):
    both = dot_tn(keys, values)
    rows = iota((2 * DK, DV), 0)
    return jnp.where(rows < DK, both[:, :DV], both[:, DV:])


def summed(where, pair):
    both = dot(jnp.where(where, 1.0, 0.0).astype(bf16), pair)
    return both[:, 0:128] + both[:, 128:256]


def packed_decays(latent_decay, context_decay):
    lanes = iota(latent_decay.shape, 1)
    lh, ll = halves(latent_decay)
    ch, cl = halves(context_decay)
    lat2 = jnp.where(lanes < 32, lh.astype(f32), ll.astype(f32))
    ctx2 = jnp.where(lanes < 96, ch.astype(f32), cl.astype(f32))
    return jnp.where(lanes < 64, lat2, ctx2)


def prepare_kernel(
    cond_l_ref, cond_c_ref, mod_ref, q_ref, k_ref, v_ref, rank_ref, out_w_ref, out_ref
):
    depth = q_ref.shape[0]

    quarter = depth // CUTS

    def put(base, array):
        scaled = array.astype(f32) * WEIGHT_SCALE
        for cut in range(CUTS):
            out_ref[cut, base : base + quarter, :] = scaled[cut * quarter : (cut + 1) * quarter]

    put(0, out_w_ref[0:depth])
    put(quarter, out_w_ref[depth : 2 * depth])
    heads = OUT_ROWS + TERM_ROWS
    put(heads, q_ref[...])
    put(heads + quarter, k_ref[...])
    put(heads + 2 * quarter, v_ref[:, 0:128])
    put(heads + 3 * quarter, v_ref[:, 128:256])
    put(heads + 4 * quarter, rank_ref[...].astype(f32).T)

    def silu(c):
        return c / (1.0 + jnp.exp(-c))

    row = iota((16, depth), 0)
    conds = jnp.where(
        row == 0, silu(cond_l_ref[...]), jnp.where(row == 1, silu(cond_c_ref[...]), 0.0)
    ).astype(bf16)
    out_ref[:, OUT_ROWS:heads, :] = jnp.zeros((CUTS, TERM_ROWS, 128), f32)
    terms = [dot(conds, mod_ref[r]) * TERM_SCALE for r in range(3)]
    vectors = [(terms[0], 0), (terms[1], 0), (terms[2], 0), (terms[0], 1), (terms[1], 1)]
    columns = mod_ref.shape[2] // 128
    lines = len(vectors) * columns
    for n, (term, at) in enumerate(vectors):
        for c in range(columns):
            line = term[at : at + 1, c * 128 : (c + 1) * 128]
            high = line.astype(bf16).astype(f32)
            spot = n * columns + c
            for at_row, value in ((spot, high), (lines + spot, line - high)):
                place = OUT_ROWS + at_row % TERM_ROWS
                out_ref[at_row // TERM_ROWS, place : place + 1, :] = value


def prepare(cond_latent, cond_context, mod_weight, w_query, w_key, w_value, w_rank, w_out):
    depth = w_query.shape[0]
    vmem = pl.BlockSpec(memory_space=pltpu.VMEM)
    ranks = jnp.swapaxes(w_rank, 1, 2).reshape(128, depth)
    return pl.pallas_call(
        prepare_kernel,
        out_shape=jax.ShapeDtypeStruct((CUTS, OUT_ROWS + TERM_ROWS + HEAD_ROWS, 128), f32),
        in_specs=[vmem] * 8,
        out_specs=vmem,
        name="prepare",
    )(
        cond_latent.reshape(1, depth), cond_context.reshape(1, depth),
        mod_weight, w_query, w_key, w_value, ranks, w_out,
    )


def stats_kernel(latent_ref, context_ref, out_ref):
    T = latent_ref.shape[0]
    C = context_ref.shape[0]
    for ref, at, size in ((latent_ref, 0, T), (context_ref, T, C)):
        x = ref[...].astype(f32)
        scale = lax.rsqrt(jnp.mean(x * x, axis=-1, keepdims=True) + eps)
        out_ref[at : at + size, :] = jnp.broadcast_to(scale, (size, 128))


def stats(latent, context):
    T, C = latent.shape[0], context.shape[0]
    vmem = pl.BlockSpec(memory_space=pltpu.VMEM)
    return pl.pallas_call(
        stats_kernel,
        out_shape=jax.ShapeDtypeStruct((T + C, 128), f32),
        in_specs=[vmem] * 2,
        out_specs=vmem,
        compiler_params=pltpu.CompilerParams(vmem_limit_bytes=VMEM_LIMIT),
        name="stats",
    )(latent, context)


def mixing_kernel(
    latent_ref, context_ref, stats_ref, rows_ref, gain_ref,
    upper_ref, lower_ref, wd_ref, bias_ref, shift_ref,
    qkv_ref, pairs_ref, send_ref, acc,
):
    step = pl.program_id(0)
    T = latent_ref.shape[0]
    C = context_ref.shape[0]
    columns = rows_ref.shape[1] // 5

    @pl.when(step == 0)
    def _():
        acc[...] = jnp.zeros_like(acc)

    def modulated(ref, at, size, shift_row, scale_row):
        parts = []
        for c in range(columns):
            cols = slice(c * 128, (c + 1) * 128)
            spot = scale_row * columns + c
            scale = gain_ref[0, :, cols] * (1.0 + rows_ref[0, spot : spot + 1, :])
            spot = shift_row * columns + c
            shift = rows_ref[0, spot : spot + 1, :]
            x = ref[:, cols].astype(f32) * stats_ref[at : at + size, :]
            parts.append((x * scale + shift).astype(bf16))
        return jnp.concatenate(parts, axis=1)

    held = [
        [
            jnp.concatenate([upper_ref[cut, j], lower_ref[cut, j]], axis=0)
            for cut in range(upper_ref.shape[0])
        ]
        for j in range(upper_ref.shape[1])
    ]
    quarter = HEAD_ROWS // 5

    def weight(n):
        rows = slice(n * quarter, (n + 1) * quarter)
        return jnp.concatenate([part[rows] for cuts in held for part in cuts], axis=0)

    w_qk = jnp.concatenate([weight(0), weight(1)], axis=1)
    w_v = jnp.concatenate([weight(2), weight(3)], axis=1)
    h = modulated(latent_ref, 0, T, 0, 1)
    hc = modulated(context_ref, T, C, 3, 4)
    h = jnp.concatenate([h, hc, jnp.zeros((acc.shape[0] - T - C, h.shape[1]), bf16)], axis=0)
    acc[:, 0:256] += dot(h, w_qk)
    acc[:, 256:512] += dot(h, w_v)
    acc[:, 512:640] += dot(h, weight(4))

    @pl.when(step == pl.num_programs(0) - 1)
    def _():
        C = acc.shape[0] - T
        unscale = 1.0 / WEIGHT_SCALE
        q16 = (acc[0:T, 0:128] * unscale).astype(bf16)
        k16 = (acc[0:T, 128:256] * unscale).astype(bf16)
        v = (acc[0:T, 256:512] * unscale).astype(bf16)
        k = k16.astype(f32)
        ranks = (acc[:, 512:640] * unscale).astype(bf16)
        rank_lane = iota(ranks.shape, 1)
        none = jnp.zeros_like(ranks)
        pre = jnp.concatenate(
            [
                dot(jnp.where(rank_lane < 64, ranks, none), wd_ref[...]) + bias_ref[0:1, :],
                dot(jnp.where(rank_lane < 64, none, ranks), wd_ref[...]) + bias_ref[1:2, :],
            ],
            axis=1,
        )
        logs = log_sigmoid(pre) / normalizer

        def down(h):
            return jnp.broadcast_to(shift_ref[h : h + 1, :], (128, T)).T

        shifts = jnp.where(iota((T, 128), 1) < DK, down(0), down(1))
        lat = logs[0:T] + jnp.concatenate([shifts, shifts], axis=1)
        qkv_ref[:, 0:128] = q16
        qkv_ref[:, 128:256] = k16
        qkv_ref[:, 256:512] = v
        f_high, f_low = halves(lat[:, 0:128])
        b_high, b_low = halves(lat[:, 128:256])
        f_pair = jnp.concatenate([f_high, f_low], axis=1)
        b_pair = jnp.concatenate([b_high, b_low], axis=1)
        pairs_ref[:, 0:256] = f_pair
        pairs_ref[:, 256:512] = b_pair
        r = iota((T, T), 0)
        s = iota((T, T), 1)
        k_f = (k * jnp.exp(summed(s > r, f_pair))).astype(bf16)
        k_b = (k * jnp.exp(summed(s < r, b_pair))).astype(bf16)

        def total(high, low):
            ones = jnp.ones((high.shape[0], 128), bf16)
            return jnp.exp(dot_tn(high, ones) + dot_tn(low, ones))

        n = send_ref.shape[0]
        slab = send_ref.shape[1] // 3
        st_f = head_state(k_f, v)
        st_b = head_state(k_b, v)
        half = n // 2
        send_ref[0:half, 0:slab, :] = st_f.reshape(half, slab, 128).astype(bf16)
        send_ref[half:n, 0:slab, :] = st_b.reshape(half, slab, 128).astype(bf16)

        crow = iota((C, 128), 0)
        live = crow < 8
        kc = jnp.where(live, (acc[T : T + C, 128:256] * unscale).astype(bf16).astype(f32), 0.0)
        vc = (acc[T : T + C, 256:512] * unscale).astype(bf16)
        ctx_f = jnp.where(live, logs[T : T + C, 0:128], 0.0)
        ctx_b = jnp.where(live, logs[T : T + C, 128:256], 0.0)
        cf_high, cf_low = halves(ctx_f)
        cb_high, cb_low = halves(ctx_b)
        rc = iota((C, C), 0)
        sc = iota((C, C), 1)
        kc_f = (kc * jnp.exp(summed(sc > rc, jnp.concatenate([cf_high, cf_low], axis=1)))).astype(bf16)
        kc_b = (kc * jnp.exp(summed(sc < rc, jnp.concatenate([cb_high, cb_low], axis=1)))).astype(bf16)
        send_ref[0:half, slab : 2 * slab, :] = head_state(kc_f, vc).reshape(half, slab, 128).astype(bf16)
        send_ref[half:n, slab : 2 * slab, :] = head_state(kc_b, vc).reshape(half, slab, 128).astype(bf16)

        def packed(latent_total, context_total):
            both = packed_decays(latent_total, context_total)
            return both.reshape(half, slab, 128).astype(bf16)

        send_ref[0:half, 2 * slab :, :] = packed(total(f_high, f_low), total(cf_high, cf_low))
        send_ref[half:n, 2 * slab :, :] = packed(total(b_high, b_low), total(cb_high, cb_low))


def mixing(
    latent, context, scales, rows, gain, gathered, w_decay, decay_bias, decay_shift
):
    T, width = latent.shape
    C = context.shape[0]
    steps = rows.shape[0]
    depth = width // steps
    whole = lambda *shape: pl.BlockSpec(shape, lambda i: (0,) * len(shape))
    return pl.pallas_call(
        mixing_kernel,
        grid=(steps,),
        in_specs=[
            pl.BlockSpec((T, depth), lambda i: (0, i)),
            pl.BlockSpec((C, depth), lambda i: (0, i)),
            whole(T + C, 128),
            pl.BlockSpec((1, *rows.shape[1:]), lambda i: (i, 0, 0)),
            pl.BlockSpec((1, 1, depth), lambda i: (i, 0, 0)),
            *[
                pl.BlockSpec(
                    (CUTS, gathered.shape[1] // steps, PART, 128),
                    lambda i, b=b: (0, i, b, 0),
                )
                for b in (1, 2)
            ],
            whole(128, 128),
            whole(2, 128),
            whole(2, T),
        ],
        out_specs=[whole(T, 512), whole(T, 512), whole(NEAR, 3 * 256 // NEAR, 128)],
        out_shape=[
            jax.ShapeDtypeStruct((T, 512), bf16),
            jax.ShapeDtypeStruct((T, 512), bf16),
            jax.ShapeDtypeStruct((NEAR, 3 * 256 // NEAR, 128), bf16),
        ],
        scratch_shapes=[pltpu.VMEM((T + 16, 640), f32)],
        compiler_params=pltpu.CompilerParams(vmem_limit_bytes=VMEM_LIMIT),
        name="mixing",
    )(
        latent, context, scales, rows, gain.reshape(steps, 1, depth), gathered, gathered,
        w_decay.reshape(128, 128), decay_bias, decay_shift.T,
    )


def scores_kernel(qkv_ref, pairs_ref, loc_ref, lift_ref):
    T = qkv_ref.shape[0]
    q16 = qkv_ref[:, 0:128]
    k16 = qkv_ref[:, 128:256]
    v = qkv_ref[:, 256:512]
    q = q16.astype(f32)
    k = k16.astype(f32)
    f_pair = pairs_ref[:, 0:256]
    b_pair = pairs_ref[:, 256:512]
    r = iota((T, T), 0)
    s = iota((T, T), 1)
    lane = iota((T, 128), 1)
    row = iota((T, 128), 0)
    first = lane < DK
    zero = jnp.zeros((T, 128), bf16)

    def scores(qs, ks):
        return (
            dot_nt(qs, jnp.where(first, ks, zero)),
            dot_nt(qs, jnp.where(first, zero, ks)),
        )

    s0, s1 = scores(q16, k16)
    s0 = 2.0 * s0
    s1 = 2.0 * s1
    m = 1
    while m < T:
        base = (r // (2 * m)) * (2 * m)
        ref = base + m
        upper = r >= ref
        lower = r < ref
        d_f = (upper & (s >= ref) & (s <= r)) | (lower & (s > r) & (s < ref))
        d_b = (upper & (s >= ref) & (s < r)) | (lower & (s >= r) & (s < ref))
        fac_f = jnp.exp(summed(d_f, f_pair))
        fac_b = jnp.exp(summed(d_b, b_pair))
        up = (row & m) != 0
        qs = (q * jnp.where(up, fac_f, fac_b)).astype(bf16)
        ks = (k * jnp.where(up, fac_b, fac_f)).astype(bf16)
        m0, m1 = scores(qs, ks)
        pick = ((r ^ s) >= m) & ((r ^ s) < 2 * m)
        s0 = jnp.where(pick, m0, s0)
        s1 = jnp.where(pick, m1, s1)
        m *= 2
    loc_ref[:, 0:128] = dot(s0.astype(bf16), v[:, 0:128])
    loc_ref[:, 128:256] = dot(s1.astype(bf16), v[:, 128:256])
    lift_ref[:, 0:128] = (q * jnp.exp(summed(s <= r, f_pair))).astype(bf16)
    lift_ref[:, 128:256] = (q * jnp.exp(summed(s >= r, b_pair))).astype(bf16)


def local_scores(qkv, pairs):
    T = qkv.shape[0]
    vmem = pl.BlockSpec(memory_space=pltpu.VMEM)
    return pl.pallas_call(
        scores_kernel,
        out_shape=[
            jax.ShapeDtypeStruct((T, 256), f32),
            jax.ShapeDtypeStruct((T, 256), bf16),
        ],
        in_specs=[vmem] * 2,
        out_specs=[vmem] * 2,
        compiler_params=pltpu.CompilerParams(vmem_limit_bytes=VMEM_LIMIT),
        cost_estimate=pl.CostEstimate(
            flops=40 * 2 * T * T * 256, bytes_accessed=T * 4096, transcendentals=20 * T * 128
        ),
        name="scores",
    )(qkv, pairs)


def slab_parts(ref, at, slab):
    rows = ref[at, 2 * slab : 3 * slab, :].astype(f32)

    def decay(lane):
        both = rows[:, lane : lane + 1] + rows[:, lane + 32 : lane + 33]
        return jnp.broadcast_to(both, (slab, 128))

    return (
        ref[at, 0:slab, :].astype(f32),
        ref[at, slab : 2 * slab, :].astype(f32),
        decay(0),
        decay(64),
    )


def ordered(backward, i, count):
    return jnp.where(backward, count - 1 - i, i)


def near_kernel(in_ref, state_ref, decay_ref, total_ref):
    n = in_ref.shape[0]
    slab = in_ref.shape[1] // 3
    backward = lax.rem(lax.axis_index("sp"), n) >= n // 2
    lat = jnp.zeros((slab, 128), f32)
    ctx = jnp.zeros((slab, 128), f32)
    lat_decay = jnp.ones((slab, 128), f32)
    ctx_decay = jnp.ones((slab, 128), f32)
    for i in range(n):
        at = ordered(backward, i, n)
        state_ref[at] = lat
        decay_ref[at] = lat_decay
        own_lat, own_ctx, dl, dc = slab_parts(in_ref, at, slab)
        lat = dl * lat + own_lat
        ctx = dc * ctx + own_ctx
        lat_decay = dl * lat_decay
        ctx_decay = dc * ctx_decay
    total_ref[0:slab, :] = lat.astype(bf16)
    total_ref[slab : 2 * slab, :] = ctx.astype(bf16)
    total_ref[2 * slab :, :] = packed_decays(lat_decay, ctx_decay).astype(bf16)


def far_kernel(totals_ref, state_ref, decay_ref, out_ref):
    groups = totals_ref.shape[0]
    n = state_ref.shape[0]
    slab = state_ref.shape[1]
    place = lax.axis_index("sp")
    backward = lax.rem(place, n) >= n // 2
    group = place // n
    mine = ordered(backward, group, groups)
    start = jnp.zeros((slab, 128), f32)
    for i in range(groups):
        _, ctx, _, dc = slab_parts(totals_ref, ordered(backward, i, groups), slab)
        start = dc * start + ctx
    for i in range(groups - 1):
        lat, _, dl, _ = slab_parts(totals_ref, ordered(backward, i, groups), slab)
        start = jnp.where(i < mine, dl * start + lat, start)
    for m in range(n):
        out_ref[m] = (decay_ref[m] * start + state_ref[m]).astype(bf16)


def states_before(sent):
    n, rows, _ = sent.shape
    slab = rows // 3
    members = lax.axis_size("sp")
    near = [list(range(i, i + n)) for i in range(0, members, n)]
    far = [list(range(i, members, n)) for i in range(n)]
    vmem = pl.BlockSpec(memory_space=pltpu.VMEM)
    received = lax.all_to_all(
        sent, "sp", split_axis=0, concat_axis=0, tiled=True, axis_index_groups=near
    )
    state, decay, total = pl.pallas_call(
        near_kernel,
        out_shape=[
            jax.ShapeDtypeStruct((n, slab, 128), f32),
            jax.ShapeDtypeStruct((n, slab, 128), f32),
            jax.ShapeDtypeStruct((rows, 128), bf16),
        ],
        in_specs=[vmem],
        out_specs=[vmem] * 3,
        name="near",
    )(received)
    totals = lax.all_gather(total, "sp", axis_index_groups=far)
    entries = pl.pallas_call(
        far_kernel,
        out_shape=jax.ShapeDtypeStruct((n, slab, 128), bf16),
        in_specs=[vmem] * 3,
        out_specs=vmem,
        name="far",
    )(totals, state, decay)
    return lax.all_to_all(
        entries, "sp", split_axis=0, concat_axis=0, tiled=True, axis_index_groups=near
    )


def normalized_output(loc_ref, lift_ref, entry_ref, gain_ref, normed):
    entry = entry_ref[...].astype(f32)
    head = (iota(entry.shape, 0) // DK) % 2
    spread = jnp.concatenate(
        [jnp.where(head == 0, entry, 0.0), jnp.where(head == 1, entry, 0.0)], axis=1
    ).astype(bf16)
    combined = loc_ref[...] + dot(lift_ref[...], spread)
    for g in range(2):
        part = combined[:, g * DV : (g + 1) * DV]
        scaled = part * lax.rsqrt(jnp.mean(part * part, axis=-1, keepdims=True) + eps)
        normed[:, g * DV : (g + 1) * DV] = (
            scaled * gain_ref[:, g * DV : (g + 1) * DV]
        ).astype(bf16)


def column(normed, w, j):
    quarter = OUT_ROWS // 2
    halves_of = [
        jnp.concatenate(
            [w[cut, j, n * quarter : (n + 1) * quarter] for cut in range(CUTS)], axis=0
        )
        for n in range(2)
    ]
    return (dot(normed[:, 0:128], halves_of[0]) + dot(normed[:, 128:256], halves_of[1])) * (
        1.0 / WEIGHT_SCALE
    )


def sent_kernel(order_ref, loc_ref, lift_ref, entry_ref, gain_ref, w_ref, normed, out_ref):
    @pl.when(pl.program_id(0) == 0)
    def _():
        normalized_output(loc_ref, lift_ref, entry_ref, gain_ref, normed)

    w = w_ref[...]
    for j in range(w.shape[1]):
        out_ref[0, :, j * 128 : (j + 1) * 128] = column(normed, w, j).astype(bf16)


def kept_kernel(order_ref, normed, received_ref, w_ref, *out_refs):
    w = w_ref[...]
    for k, out_ref in enumerate(out_refs):

        @pl.when(pl.program_id(0) == k)
        def _():
            for j in range(w.shape[1]):
                cols = slice(j * 128, (j + 1) * 128)
                out_ref[:, cols] = (
                    column(normed, w, j) + received_ref[0, :, cols].astype(f32)
                ).astype(bf16)


def constant_block(*shape):
    return pl.BlockSpec(shape, lambda i, order: (0,) * len(shape))


def sent_parts(order, loc, lift, entry, gain, gathered, width):
    T = loc.shape[0]
    chips = order.shape[0]
    return pl.pallas_call(
        sent_kernel,
        grid_spec=pltpu.PrefetchScalarGridSpec(
            num_scalar_prefetch=1,
            grid=(chips,),
            in_specs=[
                constant_block(T, 256),
                constant_block(T, 256),
                constant_block(256, 128),
                constant_block(1, 256),
                pl.BlockSpec(
                    (CUTS, width // 128, PART, 128),
                    lambda i, order: (0, order[i], 0, 0),
                ),
            ],
            out_specs=[
                constant_block(T, 256),
                pl.BlockSpec((1, T, width), lambda i, order: (i, 0, 0)),
            ],
        ),
        out_shape=[
            jax.ShapeDtypeStruct((T, 256), bf16),
            jax.ShapeDtypeStruct((chips, T, width), bf16),
        ],
        compiler_params=pltpu.CompilerParams(vmem_limit_bytes=VMEM_LIMIT),
        name="sent",
    )(order, loc, lift, entry, gain, gathered)


def kept_parts(order, normed, received, gathered, width):
    T = normed.shape[0]
    chips = order.shape[0]
    return pl.pallas_call(
        kept_kernel,
        grid_spec=pltpu.PrefetchScalarGridSpec(
            num_scalar_prefetch=1,
            grid=(chips,),
            in_specs=[
                constant_block(T, 256),
                pl.BlockSpec((1, T, width), lambda i, order: (i, 0, 0)),
                pl.BlockSpec(
                    (CUTS, width // 128, PART, 128),
                    lambda i, order: (0, order[i], 0, 0),
                ),
            ],
            out_specs=[constant_block(T, width)] * chips,
        ),
        out_shape=[jax.ShapeDtypeStruct((T, width), bf16)] * chips,
        compiler_params=pltpu.CompilerParams(vmem_limit_bytes=VMEM_LIMIT),
        name="kept",
    )(order, normed, received, gathered)


def joined_kernel(*refs):
    out_ref = refs[-1]
    pieces = refs[:-1]
    chips = len(pieces) // 2
    place = lax.axis_index("tp")
    width = pieces[0].shape[1]
    for i in range(chips):
        base = 2 * lax.rem(place // 2 + i, chips)
        for piece, core in ((pieces[i], place % 2), (pieces[chips + i], 1 - place % 2)):
            start = pl.multiple_of((base + core) * width, width)
            out_ref[:, pl.ds(start, width)] = piece[...]


def joined(pieces):
    T, width = pieces[0].shape
    vmem = pl.BlockSpec(memory_space=pltpu.VMEM)
    return pl.pallas_call(
        joined_kernel,
        out_shape=jax.ShapeDtypeStruct((T, width * len(pieces)), bf16),
        in_specs=[vmem] * len(pieces),
        out_specs=vmem,
        compiler_params=pltpu.CompilerParams(vmem_limit_bytes=VMEM_LIMIT),
        name="joined",
    )(*pieces)


def to_partner(array):
    n = lax.axis_size("tp")
    return lax.ppermute(array, "tp", [(i, i ^ 1) for i in range(n)])


def to_chip(array, ahead):
    n = lax.axis_size("tp")
    return lax.ppermute(array, "tp", [(i, (i + 2 * ahead) % n) for i in range(n)])


def local(
    latent,
    context,
    cond_latent,
    cond_context,
    mod_weight,
    norm_gain,
    w_query,
    w_key,
    w_value,
    w_rank,
    w_decay,
    decay_bias,
    decay_shift,
    out_gain,
    w_out,
):
    T, width = latent.shape
    members = lax.axis_size("sp")
    pieces = lax.axis_size("tp")
    depth = w_query.shape[0]
    own = prepare(
        cond_latent, cond_context, mod_weight, w_query, w_key, w_value, w_rank, w_out
    ).astype(f16)
    everyone = lax.all_gather(own, "sp", axis=1, tiled=True).astype(bf16)
    gathered = everyone.reshape(CUTS, members, own.shape[1], 128)
    lines = 5 * mod_weight.shape[2] // 128
    sums = gathered[:, :, OUT_ROWS : OUT_ROWS + TERM_ROWS].astype(f32).sum(axis=1).reshape(-1, 128)
    summed_terms = (sums[:lines] + sums[lines : 2 * lines]) * (1.0 / TERM_SCALE)
    rows = sent_to_all(summed_terms, "tp")
    gate = summed_terms.reshape(5, -1)[2]

    qkv, pairs, send = mixing(
        latent, context, stats(latent, context), rows, norm_gain, gathered, w_decay, decay_bias,
        decay_shift,
    )
    loc, lift = local_scores(qkv, pairs)
    entries = states_before(send)
    columns = width // pieces
    chips = pieces // 2
    place = lax.axis_index("tp")
    order = 2 * ((place // 2 + jnp.arange(chips)) % chips) + place % 2
    normed, sent = sent_parts(
        order ^ 1, loc, lift, entries.reshape(256, 128), out_gain.reshape(1, 256),
        gathered, columns,
    )
    sums = kept_parts(order, normed, to_partner(sent), gathered, columns)
    own_latent = lax.dynamic_slice_in_dim(latent, place * columns, columns, 1)
    summed = sums[0].astype(f32)
    for i in range(1, chips):
        summed = summed + to_chip(sums[i], i).astype(f32)
    mixed = (own_latent.astype(f32) + gate * summed).astype(bf16)
    mine = [mixed] + [to_chip(mixed, chips - i) for i in range(1, chips)]
    theirs = [to_partner(piece) for piece in mine]
    return joined(mine + theirs)


def solution(mesh):
    return jax.shard_map(
        local,
        mesh=mesh,
        in_specs=(
            P(("grp", "sp"), None),
            P(("grp", "sp"), None),
            P(("grp", "sp")),
            P(("grp", "sp")),
            P(None, "sp", "tp"),
            P(),
            P("sp", "tp"),
            P("sp", "tp"),
            P("sp", "tp"),
            P(None, "sp", None),
            P(None, None, "tp"),
            P(None, "tp"),
            P(("grp", "sp"), "tp"),
            P("tp"),
            P("tp", "sp"),
        ),
        out_specs=P(("grp", "sp"), None),
        check_vma=False,
    )
```

```python
import jax
import jax.numpy as jnp
from jax import lax
from jax.experimental import pallas as pl
from jax.experimental.pallas import tpu as pltpu
from jax.sharding import PartitionSpec as P

DK = 64
DV = 128
eps = 1e-06
normalizer = 16.0
f32 = jnp.float32
bf16 = jnp.bfloat16
f16 = jnp.float16
WEIGHT_SCALE = 2.0**17
TERM_SCALE = 2.0**9
CUTS = 4
OUT_ROWS = 64
TERM_ROWS = 16
HEAD_ROWS = 160
NEAR = 8
VMEM_LIMIT = 24 * 1024 * 1024
MIXING_LIMIT = 50 * 1024 * 1024


def sent_to_all(array, axis):
    copies = jnp.broadcast_to(array, (lax.axis_size(axis), *array.shape))
    return lax.all_to_all(copies, axis, split_axis=0, concat_axis=0, tiled=True)


def dot(a, b):
    return jnp.dot(a, b, preferred_element_type=f32)


def dot_nt(a, b):
    return lax.dot_general(a, b, (((1,), (1,)), ((), ())), preferred_element_type=f32)


def dot_tn(a, b):
    return lax.dot_general(a, b, (((0,), (0,)), ((), ())), preferred_element_type=f32)


def halves(x):
    high = x.astype(bf16)
    low = (x - high.astype(f32)).astype(bf16)
    return high, low


def iota(shape, dim):
    return lax.broadcasted_iota(jnp.int32, shape, dim)


def log_sigmoid(u):
    return jnp.minimum(u, 0.0) - jnp.log1p(jnp.exp(-jnp.abs(u)))


def head_state(keys, values):
    both = dot_tn(keys, values)
    rows = iota((2 * DK, DV), 0)
    return jnp.where(rows < DK, both[:, :DV], both[:, DV:])


def summed(where, pair):
    both = dot(jnp.where(where, 1.0, 0.0).astype(bf16), pair)
    return both[:, 0:128] + both[:, 128:256]


def packed_decays(latent_decay, context_decay):
    lanes = iota(latent_decay.shape, 1)
    lh, ll = halves(latent_decay)
    ch, cl = halves(context_decay)
    lat2 = jnp.where(lanes < 32, lh.astype(f32), ll.astype(f32))
    ctx2 = jnp.where(lanes < 96, ch.astype(f32), cl.astype(f32))
    return jnp.where(lanes < 64, lat2, ctx2)


def prepare_kernel(
    cond_l_ref, cond_c_ref, mod_ref, q_ref, k_ref, v_ref, rank_ref, out_w_ref, out_ref
):
    depth = q_ref.shape[0]

    quarter = depth // CUTS

    def put(base, array):
        scaled = array.astype(f32) * WEIGHT_SCALE
        for cut in range(CUTS):
            out_ref[cut, base : base + quarter, :] = scaled[cut * quarter : (cut + 1) * quarter]

    put(0, out_w_ref[0:depth])
    put(quarter, out_w_ref[depth : 2 * depth])
    heads = OUT_ROWS + TERM_ROWS
    put(heads, q_ref[...])
    put(heads + quarter, k_ref[...])
    put(heads + 2 * quarter, v_ref[:, 0:128])
    put(heads + 3 * quarter, v_ref[:, 128:256])
    put(heads + 4 * quarter, rank_ref[...].astype(f32).T)

    def silu(c):
        return c / (1.0 + jnp.exp(-c))

    row = iota((16, depth), 0)
    conds = jnp.where(
        row == 0, silu(cond_l_ref[...]), jnp.where(row == 1, silu(cond_c_ref[...]), 0.0)
    ).astype(bf16)
    out_ref[:, OUT_ROWS:heads, :] = jnp.zeros((CUTS, TERM_ROWS, 128), f32)
    terms = [dot(conds, mod_ref[r]) * TERM_SCALE for r in range(3)]
    vectors = [(terms[0], 0), (terms[1], 0), (terms[2], 0), (terms[0], 1), (terms[1], 1)]
    columns = mod_ref.shape[2] // 128
    lines = len(vectors) * columns
    for n, (term, at) in enumerate(vectors):
        for c in range(columns):
            line = term[at : at + 1, c * 128 : (c + 1) * 128]
            high = line.astype(bf16).astype(f32)
            spot = n * columns + c
            for at_row, value in ((spot, high), (lines + spot, line - high)):
                place = OUT_ROWS + at_row % TERM_ROWS
                out_ref[at_row // TERM_ROWS, place : place + 1, :] = value


def prepare(cond_latent, cond_context, mod_weight, w_query, w_key, w_value, w_rank, w_out):
    depth = w_query.shape[0]
    vmem = pl.BlockSpec(memory_space=pltpu.VMEM)
    ranks = jnp.swapaxes(w_rank, 1, 2).reshape(128, depth)
    return pl.pallas_call(
        prepare_kernel,
        out_shape=jax.ShapeDtypeStruct((CUTS, OUT_ROWS + TERM_ROWS + HEAD_ROWS, 128), f32),
        in_specs=[vmem] * 8,
        out_specs=vmem,
        name="prepare",
    )(
        cond_latent.reshape(1, depth), cond_context.reshape(1, depth),
        mod_weight, w_query, w_key, w_value, ranks, w_out,
    )


def stats_kernel(latent_ref, context_ref, out_ref):
    T = latent_ref.shape[0]
    C = context_ref.shape[0]
    for ref, at, size in ((latent_ref, 0, T), (context_ref, T, C)):
        x = ref[...].astype(f32)
        scale = lax.rsqrt(jnp.mean(x * x, axis=-1, keepdims=True) + eps)
        out_ref[at : at + size, :] = jnp.broadcast_to(scale, (size, 128))


def stats(latent, context):
    T, C = latent.shape[0], context.shape[0]
    vmem = pl.BlockSpec(memory_space=pltpu.VMEM)
    return pl.pallas_call(
        stats_kernel,
        out_shape=jax.ShapeDtypeStruct((T + C, 128), f32),
        in_specs=[vmem] * 2,
        out_specs=vmem,
        compiler_params=pltpu.CompilerParams(vmem_limit_bytes=VMEM_LIMIT),
        name="stats",
    )(latent, context)


def mixing_kernel(
    latent_ref, context_ref, stats_ref, rows_ref, gain_ref,
    weight_ref, wd_ref, bias_ref, shift_ref,
    qkv_ref, pairs_ref, send_ref, acc,
):
    step = pl.program_id(0)
    T = latent_ref.shape[0]
    C = context_ref.shape[0]
    columns = rows_ref.shape[1] // 5

    @pl.when(step == 0)
    def _():
        acc[...] = jnp.zeros_like(acc)

    def modulated(ref, at, size, shift_row, scale_row):
        parts = []
        for c in range(columns):
            cols = slice(c * 128, (c + 1) * 128)
            spot = scale_row * columns + c
            scale = gain_ref[0, :, cols] * (1.0 + rows_ref[0, spot : spot + 1, :])
            spot = shift_row * columns + c
            shift = rows_ref[0, spot : spot + 1, :]
            x = ref[:, cols].astype(f32) * stats_ref[at : at + size, :]
            parts.append((x * scale + shift).astype(bf16))
        return jnp.concatenate(parts, axis=1)

    quarter = HEAD_ROWS // 5

    def weight(n):
        rows = slice(n * quarter, (n + 1) * quarter)
        return jnp.concatenate(
            [
                weight_ref[cut, j, rows]
                for j in range(weight_ref.shape[1])
                for cut in range(weight_ref.shape[0])
            ],
            axis=0,
        )

    w_qk = jnp.concatenate([weight(0), weight(1)], axis=1)
    w_v = jnp.concatenate([weight(2), weight(3)], axis=1)
    h = modulated(latent_ref, 0, T, 0, 1)
    hc = modulated(context_ref, T, C, 3, 4)
    h = jnp.concatenate([h, hc, jnp.zeros((acc.shape[0] - T - C, h.shape[1]), bf16)], axis=0)
    acc[:, 0:256] += dot(h, w_qk)
    acc[:, 256:512] += dot(h, w_v)
    acc[:, 512:640] += dot(h, weight(4))

    @pl.when(step == pl.num_programs(0) - 1)
    def _():
        C = acc.shape[0] - T
        unscale = 1.0 / WEIGHT_SCALE
        q16 = (acc[0:T, 0:128] * unscale).astype(bf16)
        k16 = (acc[0:T, 128:256] * unscale).astype(bf16)
        v = (acc[0:T, 256:512] * unscale).astype(bf16)
        k = k16.astype(f32)
        ranks = (acc[:, 512:640] * unscale).astype(bf16)
        rank_lane = iota(ranks.shape, 1)
        none = jnp.zeros_like(ranks)
        pre = jnp.concatenate(
            [
                dot(jnp.where(rank_lane < 64, ranks, none), wd_ref[...]) + bias_ref[0:1, :],
                dot(jnp.where(rank_lane < 64, none, ranks), wd_ref[...]) + bias_ref[1:2, :],
            ],
            axis=1,
        )
        logs = log_sigmoid(pre) / normalizer

        def down(h):
            return jnp.broadcast_to(shift_ref[h : h + 1, :], (128, T)).T

        shifts = jnp.where(iota((T, 128), 1) < DK, down(0), down(1))
        lat = logs[0:T] + jnp.concatenate([shifts, shifts], axis=1)
        qkv_ref[:, 0:128] = q16
        qkv_ref[:, 128:256] = k16
        qkv_ref[:, 256:512] = v
        f_high, f_low = halves(lat[:, 0:128])
        b_high, b_low = halves(lat[:, 128:256])
        f_pair = jnp.concatenate([f_high, f_low], axis=1)
        b_pair = jnp.concatenate([b_high, b_low], axis=1)
        pairs_ref[:, 0:256] = f_pair
        pairs_ref[:, 256:512] = b_pair
        r = iota((T, T), 0)
        s = iota((T, T), 1)
        k_f = (k * jnp.exp(summed(s > r, f_pair))).astype(bf16)
        k_b = (k * jnp.exp(summed(s < r, b_pair))).astype(bf16)

        def total(high, low):
            ones = jnp.ones((high.shape[0], 128), bf16)
            return jnp.exp(dot_tn(high, ones) + dot_tn(low, ones))

        n = send_ref.shape[0]
        slab = send_ref.shape[1] // 3
        st_f = head_state(k_f, v)
        st_b = head_state(k_b, v)
        half = n // 2
        send_ref[0:half, 0:slab, :] = st_f.reshape(half, slab, 128).astype(bf16)
        send_ref[half:n, 0:slab, :] = st_b.reshape(half, slab, 128).astype(bf16)

        crow = iota((C, 128), 0)
        live = crow < 8
        kc = jnp.where(live, (acc[T : T + C, 128:256] * unscale).astype(bf16).astype(f32), 0.0)
        vc = (acc[T : T + C, 256:512] * unscale).astype(bf16)
        ctx_f = jnp.where(live, logs[T : T + C, 0:128], 0.0)
        ctx_b = jnp.where(live, logs[T : T + C, 128:256], 0.0)
        cf_high, cf_low = halves(ctx_f)
        cb_high, cb_low = halves(ctx_b)
        rc = iota((C, C), 0)
        sc = iota((C, C), 1)
        kc_f = (kc * jnp.exp(summed(sc > rc, jnp.concatenate([cf_high, cf_low], axis=1)))).astype(bf16)
        kc_b = (kc * jnp.exp(summed(sc < rc, jnp.concatenate([cb_high, cb_low], axis=1)))).astype(bf16)
        send_ref[0:half, slab : 2 * slab, :] = head_state(kc_f, vc).reshape(half, slab, 128).astype(bf16)
        send_ref[half:n, slab : 2 * slab, :] = head_state(kc_b, vc).reshape(half, slab, 128).astype(bf16)

        def packed(latent_total, context_total):
            both = packed_decays(latent_total, context_total)
            return both.reshape(half, slab, 128).astype(bf16)

        send_ref[0:half, 2 * slab :, :] = packed(total(f_high, f_low), total(cf_high, cf_low))
        send_ref[half:n, 2 * slab :, :] = packed(total(b_high, b_low), total(cb_high, cb_low))


def mixing(
    latent, context, scales, rows, gain, gathered, w_decay, decay_bias, decay_shift
):
    T, width = latent.shape
    C = context.shape[0]
    steps = rows.shape[0]
    depth = width // steps
    whole = lambda *shape: pl.BlockSpec(shape, lambda i: (0,) * len(shape))
    return pl.pallas_call(
        mixing_kernel,
        grid=(steps,),
        in_specs=[
            pl.BlockSpec((T, depth), lambda i: (0, i)),
            pl.BlockSpec((C, depth), lambda i: (0, i)),
            whole(T + C, 128),
            pl.BlockSpec((1, *rows.shape[1:]), lambda i: (i, 0, 0)),
            pl.BlockSpec((1, 1, depth), lambda i: (i, 0, 0)),
            pl.BlockSpec(
                (CUTS, gathered.shape[1] // steps, HEAD_ROWS, 128), lambda i: (0, i, 0, 0)
            ),
            whole(128, 128),
            whole(2, 128),
            whole(2, T),
        ],
        out_specs=[whole(T, 512), whole(T, 512), whole(NEAR, 3 * 256 // NEAR, 128)],
        out_shape=[
            jax.ShapeDtypeStruct((T, 512), bf16),
            jax.ShapeDtypeStruct((T, 512), bf16),
            jax.ShapeDtypeStruct((NEAR, 3 * 256 // NEAR, 128), bf16),
        ],
        scratch_shapes=[pltpu.VMEM((T + 16, 640), f32)],
        compiler_params=pltpu.CompilerParams(vmem_limit_bytes=MIXING_LIMIT),
        name="mixing",
    )(
        latent, context, scales, rows, gain.reshape(steps, 1, depth), gathered,
        w_decay.reshape(128, 128), decay_bias, decay_shift.T,
    )


def scores_kernel(qkv_ref, pairs_ref, loc_ref, lift_ref):
    T = qkv_ref.shape[0]
    q16 = qkv_ref[:, 0:128]
    k16 = qkv_ref[:, 128:256]
    v = qkv_ref[:, 256:512]
    q = q16.astype(f32)
    k = k16.astype(f32)
    f_pair = pairs_ref[:, 0:256]
    b_pair = pairs_ref[:, 256:512]
    r = iota((T, T), 0)
    s = iota((T, T), 1)
    lane = iota((T, 128), 1)
    row = iota((T, 128), 0)
    first = lane < DK
    zero = jnp.zeros((T, 128), bf16)

    def scores(qs, ks):
        return (
            dot_nt(qs, jnp.where(first, ks, zero)),
            dot_nt(qs, jnp.where(first, zero, ks)),
        )

    s0, s1 = scores(q16, k16)
    s0 = 2.0 * s0
    s1 = 2.0 * s1
    m = 1
    while m < T:
        base = (r // (2 * m)) * (2 * m)
        ref = base + m
        upper = r >= ref
        lower = r < ref
        d_f = (upper & (s >= ref) & (s <= r)) | (lower & (s > r) & (s < ref))
        d_b = (upper & (s >= ref) & (s < r)) | (lower & (s >= r) & (s < ref))
        fac_f = jnp.exp(summed(d_f, f_pair))
        fac_b = jnp.exp(summed(d_b, b_pair))
        up = (row & m) != 0
        qs = (q * jnp.where(up, fac_f, fac_b)).astype(bf16)
        ks = (k * jnp.where(up, fac_b, fac_f)).astype(bf16)
        m0, m1 = scores(qs, ks)
        pick = ((r ^ s) >= m) & ((r ^ s) < 2 * m)
        s0 = jnp.where(pick, m0, s0)
        s1 = jnp.where(pick, m1, s1)
        m *= 2
    loc_ref[:, 0:128] = dot(s0.astype(bf16), v[:, 0:128])
    loc_ref[:, 128:256] = dot(s1.astype(bf16), v[:, 128:256])
    lift_ref[:, 0:128] = (q * jnp.exp(summed(s <= r, f_pair))).astype(bf16)
    lift_ref[:, 128:256] = (q * jnp.exp(summed(s >= r, b_pair))).astype(bf16)


def local_scores(qkv, pairs):
    T = qkv.shape[0]
    vmem = pl.BlockSpec(memory_space=pltpu.VMEM)
    return pl.pallas_call(
        scores_kernel,
        out_shape=[
            jax.ShapeDtypeStruct((T, 256), f32),
            jax.ShapeDtypeStruct((T, 256), bf16),
        ],
        in_specs=[vmem] * 2,
        out_specs=[vmem] * 2,
        compiler_params=pltpu.CompilerParams(vmem_limit_bytes=VMEM_LIMIT),
        cost_estimate=pl.CostEstimate(
            flops=40 * 2 * T * T * 256, bytes_accessed=T * 4096, transcendentals=20 * T * 128
        ),
        name="scores",
    )(qkv, pairs)


def slab_parts(ref, at, slab):
    rows = ref[at, 2 * slab : 3 * slab, :].astype(f32)

    def decay(lane):
        both = rows[:, lane : lane + 1] + rows[:, lane + 32 : lane + 33]
        return jnp.broadcast_to(both, (slab, 128))

    return (
        ref[at, 0:slab, :].astype(f32),
        ref[at, slab : 2 * slab, :].astype(f32),
        decay(0),
        decay(64),
    )


def ordered(backward, i, count):
    return jnp.where(backward, count - 1 - i, i)


def near_kernel(in_ref, state_ref, decay_ref, total_ref):
    n = in_ref.shape[0]
    slab = in_ref.shape[1] // 3
    backward = lax.rem(lax.axis_index("sp"), n) >= n // 2
    lat = jnp.zeros((slab, 128), f32)
    ctx = jnp.zeros((slab, 128), f32)
    lat_decay = jnp.ones((slab, 128), f32)
    ctx_decay = jnp.ones((slab, 128), f32)
    for i in range(n):
        at = ordered(backward, i, n)
        state_ref[at] = lat
        decay_ref[at] = lat_decay
        own_lat, own_ctx, dl, dc = slab_parts(in_ref, at, slab)
        lat = dl * lat + own_lat
        ctx = dc * ctx + own_ctx
        lat_decay = dl * lat_decay
        ctx_decay = dc * ctx_decay
    total_ref[0:slab, :] = lat.astype(bf16)
    total_ref[slab : 2 * slab, :] = ctx.astype(bf16)
    total_ref[2 * slab :, :] = packed_decays(lat_decay, ctx_decay).astype(bf16)


def far_kernel(totals_ref, state_ref, decay_ref, out_ref):
    groups = totals_ref.shape[0]
    n = state_ref.shape[0]
    slab = state_ref.shape[1]
    place = lax.axis_index("sp")
    backward = lax.rem(place, n) >= n // 2
    group = place // n
    mine = ordered(backward, group, groups)
    start = jnp.zeros((slab, 128), f32)
    for i in range(groups):
        _, ctx, _, dc = slab_parts(totals_ref, ordered(backward, i, groups), slab)
        start = dc * start + ctx
    for i in range(groups - 1):
        lat, _, dl, _ = slab_parts(totals_ref, ordered(backward, i, groups), slab)
        start = jnp.where(i < mine, dl * start + lat, start)
    for m in range(n):
        out_ref[m] = (decay_ref[m] * start + state_ref[m]).astype(bf16)


def states_before(sent):
    n, rows, _ = sent.shape
    slab = rows // 3
    members = lax.axis_size("sp")
    near = [list(range(i, i + n)) for i in range(0, members, n)]
    far = [list(range(i, members, n)) for i in range(n)]
    vmem = pl.BlockSpec(memory_space=pltpu.VMEM)
    received = lax.all_to_all(
        sent, "sp", split_axis=0, concat_axis=0, tiled=True, axis_index_groups=near
    )
    state, decay, total = pl.pallas_call(
        near_kernel,
        out_shape=[
            jax.ShapeDtypeStruct((n, slab, 128), f32),
            jax.ShapeDtypeStruct((n, slab, 128), f32),
            jax.ShapeDtypeStruct((rows, 128), bf16),
        ],
        in_specs=[vmem],
        out_specs=[vmem] * 3,
        compiler_params=pltpu.CompilerParams(vmem_limit_bytes=VMEM_LIMIT),
        name="near",
    )(received)
    totals = lax.all_gather(total, "sp", axis_index_groups=far)
    entries = pl.pallas_call(
        far_kernel,
        out_shape=jax.ShapeDtypeStruct((n, slab, 128), bf16),
        in_specs=[vmem] * 3,
        out_specs=vmem,
        compiler_params=pltpu.CompilerParams(vmem_limit_bytes=VMEM_LIMIT),
        name="far",
    )(totals, state, decay)
    return lax.all_to_all(
        entries, "sp", split_axis=0, concat_axis=0, tiled=True, axis_index_groups=near
    )


def normalized_output(loc_ref, lift_ref, entry_ref, gain_ref, normed):
    entry = entry_ref[...].astype(f32)
    head = (iota(entry.shape, 0) // DK) % 2
    spread = jnp.concatenate(
        [jnp.where(head == 0, entry, 0.0), jnp.where(head == 1, entry, 0.0)], axis=1
    ).astype(bf16)
    combined = loc_ref[...] + dot(lift_ref[...], spread)
    for g in range(2):
        part = combined[:, g * DV : (g + 1) * DV]
        scaled = part * lax.rsqrt(jnp.mean(part * part, axis=-1, keepdims=True) + eps)
        normed[:, g * DV : (g + 1) * DV] = (
            scaled * gain_ref[:, g * DV : (g + 1) * DV]
        ).astype(bf16)


def column(normed, w, j):
    quarter = OUT_ROWS // 2
    halves_of = [
        jnp.concatenate(
            [w[cut, j, n * quarter : (n + 1) * quarter] for cut in range(CUTS)], axis=0
        )
        for n in range(2)
    ]
    return (dot(normed[:, 0:128], halves_of[0]) + dot(normed[:, 128:256], halves_of[1])) * (
        1.0 / WEIGHT_SCALE
    )


def sent_kernel(order_ref, loc_ref, lift_ref, entry_ref, gain_ref, w_ref, normed, out_ref):
    @pl.when(pl.program_id(0) == 0)
    def _():
        normalized_output(loc_ref, lift_ref, entry_ref, gain_ref, normed)

    w = w_ref[...]
    for j in range(w.shape[1]):
        out_ref[0, :, j * 128 : (j + 1) * 128] = column(normed, w, j).astype(bf16)


def kept_kernel(order_ref, normed, received_ref, w_ref, *out_refs):
    w = w_ref[...]
    for k, out_ref in enumerate(out_refs):

        @pl.when(pl.program_id(0) == k)
        def _():
            for j in range(w.shape[1]):
                cols = slice(j * 128, (j + 1) * 128)
                out_ref[:, cols] = (
                    column(normed, w, j) + received_ref[0, :, cols].astype(f32)
                ).astype(bf16)


def constant_block(*shape):
    return pl.BlockSpec(shape, lambda i, order: (0,) * len(shape))


def sent_parts(order, loc, lift, entry, gain, gathered, width):
    T = loc.shape[0]
    chips = order.shape[0]
    return pl.pallas_call(
        sent_kernel,
        grid_spec=pltpu.PrefetchScalarGridSpec(
            num_scalar_prefetch=1,
            grid=(chips,),
            in_specs=[
                constant_block(T, 256),
                constant_block(T, 256),
                constant_block(256, 128),
                constant_block(1, 256),
                pl.BlockSpec(
                    (CUTS, width // 128, OUT_ROWS, 128),
                    lambda i, order: (0, order[i], 0, 0),
                ),
            ],
            out_specs=[
                constant_block(T, 256),
                pl.BlockSpec((1, T, width), lambda i, order: (i, 0, 0)),
            ],
        ),
        out_shape=[
            jax.ShapeDtypeStruct((T, 256), bf16),
            jax.ShapeDtypeStruct((chips, T, width), bf16),
        ],
        compiler_params=pltpu.CompilerParams(vmem_limit_bytes=VMEM_LIMIT),
        name="sent",
    )(order, loc, lift, entry, gain, gathered)


def kept_parts(order, normed, received, gathered, width):
    T = normed.shape[0]
    chips = order.shape[0]
    return pl.pallas_call(
        kept_kernel,
        grid_spec=pltpu.PrefetchScalarGridSpec(
            num_scalar_prefetch=1,
            grid=(chips,),
            in_specs=[
                constant_block(T, 256),
                pl.BlockSpec((1, T, width), lambda i, order: (i, 0, 0)),
                pl.BlockSpec(
                    (CUTS, width // 128, OUT_ROWS, 128),
                    lambda i, order: (0, order[i], 0, 0),
                ),
            ],
            out_specs=[constant_block(T, width)] * chips,
        ),
        out_shape=[jax.ShapeDtypeStruct((T, width), bf16)] * chips,
        compiler_params=pltpu.CompilerParams(vmem_limit_bytes=VMEM_LIMIT),
        name="kept",
    )(order, normed, received, gathered)


def joined_kernel(*refs):
    out_ref = refs[-1]
    pieces = refs[:-1]
    chips = len(pieces) // 2
    place = lax.axis_index("tp")
    width = pieces[0].shape[1]
    for i in range(chips):
        base = 2 * lax.rem(place // 2 + i, chips)
        for piece, core in ((pieces[i], place % 2), (pieces[chips + i], 1 - place % 2)):
            start = pl.multiple_of((base + core) * width, width)
            out_ref[:, pl.ds(start, width)] = piece[...]


def joined(pieces):
    T, width = pieces[0].shape
    vmem = pl.BlockSpec(memory_space=pltpu.VMEM)
    return pl.pallas_call(
        joined_kernel,
        out_shape=jax.ShapeDtypeStruct((T, width * len(pieces)), bf16),
        in_specs=[vmem] * len(pieces),
        out_specs=vmem,
        compiler_params=pltpu.CompilerParams(vmem_limit_bytes=VMEM_LIMIT),
        name="joined",
    )(*pieces)


def to_partner(array):
    n = lax.axis_size("tp")
    return lax.ppermute(array, "tp", [(i, i ^ 1) for i in range(n)])


def to_chip(array, ahead):
    n = lax.axis_size("tp")
    return lax.ppermute(array, "tp", [(i, (i + 2 * ahead) % n) for i in range(n)])


def local(
    latent,
    context,
    cond_latent,
    cond_context,
    mod_weight,
    norm_gain,
    w_query,
    w_key,
    w_value,
    w_rank,
    w_decay,
    decay_bias,
    decay_shift,
    out_gain,
    w_out,
):
    T, width = latent.shape
    members = lax.axis_size("sp")
    pieces = lax.axis_size("tp")
    depth = w_query.shape[0]
    own = prepare(
        cond_latent, cond_context, mod_weight, w_query, w_key, w_value, w_rank, w_out
    ).astype(f16)
    everyone = lax.all_gather(own, "sp", axis=1, tiled=True)
    everyone = everyone.reshape(CUTS, members, own.shape[1], 128)
    heads = OUT_ROWS + TERM_ROWS
    lines = 5 * mod_weight.shape[2] // 128
    sums = everyone[:, :, OUT_ROWS:heads].astype(f32).sum(axis=1).reshape(-1, 128)
    summed_terms = (sums[:lines] + sums[lines : 2 * lines]) * (1.0 / TERM_SCALE)
    out_gathered = everyone[:, :, :OUT_ROWS].astype(bf16)
    gathered = everyone[:, :, heads:].astype(bf16)
    rows = sent_to_all(summed_terms, "tp")
    gate = summed_terms.reshape(5, -1)[2]

    qkv, pairs, send = mixing(
        latent, context, stats(latent, context), rows, norm_gain, gathered, w_decay, decay_bias,
        decay_shift,
    )
    loc, lift = local_scores(qkv, pairs)
    entries = states_before(send)
    columns = width // pieces
    chips = pieces // 2
    place = lax.axis_index("tp")
    order = 2 * ((place // 2 + jnp.arange(chips)) % chips) + place % 2
    normed, sent = sent_parts(
        order ^ 1, loc, lift, entries.reshape(256, 128), out_gain.reshape(1, 256),
        out_gathered, columns,
    )
    sums = kept_parts(order, normed, to_partner(sent), out_gathered, columns)
    own_latent = lax.dynamic_slice_in_dim(latent, place * columns, columns, 1)
    summed = sums[0].astype(f32)
    for i in range(1, chips):
        summed = summed + to_chip(sums[i], i).astype(f32)
    mixed = (own_latent.astype(f32) + gate * summed).astype(bf16)
    mine = [mixed] + [to_chip(mixed, chips - i) for i in range(1, chips)]
    theirs = [to_partner(piece) for piece in mine]
    return joined(mine + theirs)


def solution(mesh):
    return jax.shard_map(
        local,
        mesh=mesh,
        in_specs=(
            P(("grp", "sp"), None),
            P(("grp", "sp"), None),
            P(("grp", "sp")),
            P(("grp", "sp")),
            P(None, "sp", "tp"),
            P(),
            P("sp", "tp"),
            P("sp", "tp"),
            P("sp", "tp"),
            P(None, "sp", None),
            P(None, None, "tp"),
            P(None, "tp"),
            P(("grp", "sp"), "tp"),
            P("tp"),
            P("tp", "sp"),
        ),
        out_specs=P(("grp", "sp"), None),
        check_vma=False,
    )
```
